32 devices in a mesh: ep: 8 (over z, x), tp: 4 (over y, core).
Axes of the slice: x: 2, y: 2, z: 4, core: 2. Of those that a mesh axis runs over, the one named last changes fastest.
Arguments:
- queries: bfloat16 [2048, 2, 1024], P('ep', None, 'tp')
- keys: bfloat16 [2048, 2, 256], P('ep', None, 'tp')
- values: bfloat16 [2048, 2, 256], P('ep', None, 'tp'), may hold values from -6 to 6
- query_gain: float32 [64], replicated, may hold values from 1.2 to 6
- key_gain: float32 [64], replicated, may hold values from 1.2 to 6
- out_weight: bfloat16 [1024, 2048], P('tp'), may hold values from -0.75 to 0.75
- moe_tokens: bfloat16 [4096, 2048], P(('ep', 'tp')), may hold values from -6 to 6
- moe_gain: float32 [2048], replicated, may hold values from 0.1 to 1.9
- routes: int32 [4096, 2], P(('ep', 'tp')), may hold values from 0 to 7, all different within a row; in each aligned block of 128 rows (0 to 127, 128 to 255, ...) at most 48 rows name the same one
- route_weight: float32 [4096, 2], P(('ep', 'tp')), may hold values from 0.1 to 1
- w_gate: bfloat16 [8, 2048, 1024], P('ep', None, 'tp'), may hold values from -0.125 to 0.125
- w_up: bfloat16 [8, 2048, 1024], P('ep', None, 'tp'), may hold values from -0.125 to 0.125
- w_down: bfloat16 [8, 1024, 2048], P('ep', 'tp'), may hold values from -0.1875 to 0.1875
Outputs:
- attended: bfloat16 [2048, 2, 2048], P(('ep', 'tp'))
- routed: bfloat16 [4096, 2048], P(('ep', 'tp'))
The draws below stay inside these ranges and needn't reach their ends.
Inputs may be any that keep to these rules, and one draw needn't show every extreme that they name: `routes`: each row names 2 different experts. The rows of one device name no expert more than 48 times, and in every draw some device's rows name one expert exactly 48 times.
All inputs are finite; a program needn't handle non-finite values.
Results may differ from the reference program's by a relative error of at most 0.013.
The reference program's roundings to bfloat16 on the way count: a program that leaves them out, or rounds other values in their place, can miss the bound.
Values may be sent and summed in bfloat16 or wider, within the bound.
A program may use at most 128 MiB of HBM per device.

```python
import math
import jax
import jax.numpy as jnp
import numpy as np
from jax import lax

D = 2048
HEADS = 16
KV_HEADS = 4
HEAD_DIM = 64
FF = 1024
TOPK = 2
GRID_W = 64
SEQS = 2
TOK_DEV = 128
LEN = 2048
EXPERTS = 8
CAP = 48
TOKENS = 4096
N_EP = 8
N_TP = 4


def draw_both(key):
    keys_drawn = jax.random.normal(jax.random.fold_in(key, 12), (LEN, SEQS, KV_HEADS * HEAD_DIM), jnp.float32)
    queries_drawn = jax.random.normal(jax.random.fold_in(key, 11), (LEN, SEQS, HEADS * HEAD_DIM), jnp.float32)
    return (queries_drawn, keys_drawn)


def draw_queries(key, part):
    return draw_both(key)[0].astype(jnp.bfloat16)


def draw_keys(key, part):
    return draw_both(key)[1].astype(jnp.bfloat16)


def draw_gain_values(key):
    return jax.random.uniform(key, (HEAD_DIM,), jnp.float32, 1.2, 2.0)


def draw_query_gain(key, part):
    return draw_gain_values(jax.random.fold_in(key, 21))


def draw_key_gain(key, part):
    return draw_gain_values(jax.random.fold_in(key, 22))


def shard_levels(own_key, shape, split, least, high):
    def one(position, blocks):
        draws = jax.random.uniform(jax.random.fold_in(jax.random.fold_in(own_key, 6), position), (blocks,), jnp.float32, least / len(split), high / len(split))
        return jnp.repeat(jnp.exp(draws), shape[position] // blocks).reshape((-1,) + (1,) * (len(shape) - position - 1))

    level = one(*split[0])
    for cut in split[1:]:
        level = level * one(*cut)
    return level


def shared_out(key, own, number, rows, count, top, limit, skew):
    order = jax.random.permutation(key, count)
    heavy_load, common = load_shares(count, rows * top, limit, skew, True), load_shares(count, rows * top, limit, skew, False)
    places = jnp.arange(count)

    def named(sizes, turn):
        used = int((sizes > 0).sum())
        fixed = max(1, used // 4)
        passed = fixed + (places - fixed + turn * (used - fixed)) % max(1, count - fixed)
        return jnp.zeros((count,), jnp.int32).at[order[jnp.where(places < fixed, places, passed)]].set(jnp.asarray(sizes, jnp.int32))

    sizes = jnp.where(number % 4 == 0, named(heavy_load, number // 4), named(common, number - number // 4 - 1))
    mixed = jax.random.permutation(jax.random.fold_in(own, 3), count)
    source_of, sink = mixed[0:count // 2 * 2:2], mixed[1:count // 2 * 2:2]
    margin = jnp.minimum(sizes[source_of] - 1, limit - sizes[sink]) // 2
    margin = jnp.where((source_of == order[0]) | (sink == order[0]) | (sizes[sink] == 0), 0, jnp.maximum(margin, 0))
    passed = jax.random.randint(jax.random.fold_in(own, 4), (count // 2,), 0, 1 << 20) % (margin + 1)
    sizes = sizes.at[source_of].add(-passed).at[sink].add(passed)
    members = jnp.searchsorted(jnp.cumsum(sizes), jnp.arange(rows * top), side="right").astype(jnp.int32)
    table = members.reshape(top, rows).T
    table = table[jax.random.permutation(jax.random.fold_in(own, 1), rows)]
    turn = jax.random.randint(jax.random.fold_in(own, 2), (rows, 1), 0, top)
    return jnp.take_along_axis(table, (jnp.arange(top)[None, :] + turn) % top, axis=1)


def load_shares(number_of, total, most, slope, full):
    weights = [(1 << 20) // math.isqrt(standing ** slope) + 1 for standing in range(1, number_of + 1)]
    largest = most if full else min(most, max(-(-total // number_of), total * weights[0] // sum(weights)))
    least = 1 if total - largest >= number_of - 1 else 0
    counts, spare = [largest] + [least] * (number_of - 1), total - largest - least * (number_of - 1)
    while spare > 0:
        movable = [i for i in range(1, number_of) if counts[i] < largest] or [i for i in range(1, number_of) if counts[i] < most]
        whole, budget = sum([weights[i] for i in movable]), spare
        for i in movable:
            addition = min(most - counts[i], max(1, budget * weights[i] // whole), spare)
            counts[i] = counts[i] + addition
            spare = spare - addition
    return np.array(counts)


def normal_values(rng, shape, scale, limit, cuts=(), held_as=jnp.bfloat16):
    result = scale * jax.random.normal(rng, shape, jnp.float32)
    if cuts:
        result = result * shard_levels(rng, shape, cuts, -0.22, 0.18)
    return jnp.clip(result, -limit, limit).astype(held_as)


def setup_inputs(seed: int = 0) -> dict:
    seeds = jax.random.split(jax.random.key(seed), 14)
    queries = draw_queries(jax.random.fold_in(seeds[13], 71), 0)
    keys = draw_keys(jax.random.fold_in(seeds[13], 71), 0)
    values = normal_values(seeds[2], (LEN, SEQS, KV_HEADS * HEAD_DIM), 1.0, 6.0, ((0, 8), (2, 4)))
    query_gain = draw_query_gain(jax.random.fold_in(seeds[13], 71), 0)
    key_gain = draw_key_gain(jax.random.fold_in(seeds[13], 71), 0)
    out_weight = normal_values(seeds[5], (HEADS * HEAD_DIM, D), (HEADS * HEAD_DIM // 16) ** -0.5, 0.75, ((0, 4),))
    moe_tokens = normal_values(seeds[6], (TOKENS, D), 1.0, 6.0, ((0, 32),))
    moe_gain = jnp.clip(1.0 + 0.18 * jax.random.normal(seeds[7], (D,), jnp.float32), 0.1, 1.9)
    routes_keys = jax.random.split(jax.random.fold_in(seeds[8], 1), TOKENS // TOK_DEV)
    routes_turns = jax.random.permutation(jax.random.fold_in(seeds[8], 3), TOKENS // TOK_DEV)
    routes = jax.vmap(lambda own, number: shared_out(jax.random.fold_in(seeds[8], 2), own, number, TOK_DEV, EXPERTS, TOPK, CAP, 1))(routes_keys, routes_turns).reshape((TOKENS, TOPK))
    route_weight = jnp.clip(0.1 + 0.9 * jax.random.uniform(seeds[9], (TOKENS, TOPK), jnp.float32) ** shard_levels(seeds[9], (TOKENS, TOPK), ((0, 32),), -0.2, 0.2), 0.1, 1.0)
    w_gate = normal_values(seeds[10], (EXPERTS, D, FF), D ** -0.5, 0.125, ((0, 8), (2, 4)))
    w_up = normal_values(seeds[11], (EXPERTS, D, FF), D ** -0.5, 0.125, ((0, 8), (2, 4)))
    w_down = normal_values(seeds[12], (EXPERTS, FF, D), FF ** -0.5, 0.1875, ((0, 8), (1, 4)))
    return dict(queries=queries, keys=keys, values=values, query_gain=query_gain, key_gain=key_gain, out_weight=out_weight, moe_tokens=moe_tokens, moe_gain=moe_gain, routes=routes, route_weight=route_weight, w_gate=w_gate, w_up=w_up, w_down=w_down)


EPS = 1e-06
THETA = 10000.0

def turn(normed, positions):
    quarter = normed.shape[-1] // 4
    inverse = THETA ** (-jnp.arange(quarter, dtype=jnp.float32) / quarter)
    grid_row = (positions // GRID_W).astype(jnp.float32)
    grid_col = (positions % GRID_W).astype(jnp.float32)
    angles = jnp.stack([grid_row[:, None] * inverse, grid_col[:, None] * inverse], axis=1)
    cosine = jnp.cos(angles)[:, None, None]
    sine = jnp.sin(angles)[:, None, None]
    parts = normed.reshape(normed.shape[:-1] + (2, 2, quarter))
    first = parts[..., 0, :]
    second = parts[..., 1, :]
    turned = jnp.stack([first * cosine - second * sine, second * cosine + first * sine], axis=-2)
    return turned.reshape(normed.shape)

def prepare(data, positions, gain):
    heads = data.astype(jnp.float32).reshape(data.shape[0], data.shape[1], -1, HEAD_DIM)
    normed = heads * lax.rsqrt(lax.optimization_barrier(jnp.mean(heads * heads, axis=-1, keepdims=True)) + EPS) * gain
    return turn(normed, positions).astype(jnp.bfloat16)

def reference(queries, keys, values, query_gain, key_gain, out_weight, moe_tokens, moe_gain, routes, route_weight, w_gate, w_up, w_down):
    positions = jnp.arange(LEN, dtype=jnp.int32)
    q_rot = prepare(queries, positions, query_gain)
    k_rot = prepare(keys, positions, key_gain)
    key_float = k_rot.astype(jnp.float32)
    value_float = values.reshape(LEN, SEQS, KV_HEADS, HEAD_DIM).astype(jnp.float32)
    groups = HEADS // KV_HEADS
    block = math.gcd(LEN, 64)
    query_blocks = q_rot.reshape(LEN // block, block, SEQS, KV_HEADS, groups, HEAD_DIM)

    def attend(query_block):
        scores = jnp.einsum('bskgd,lskd->skgbl', query_block.astype(jnp.float32), key_float) * HEAD_DIM ** (-0.5)
        largest = lax.optimization_barrier(jnp.max(scores, axis=-1, keepdims=True))
        expo = jnp.exp(scores - largest)
        total = lax.optimization_barrier(jnp.sum(expo, axis=-1))
        probs = lax.optimization_barrier(expo.astype(jnp.bfloat16)).astype(jnp.float32)
        summed = jnp.einsum('skgbl,lskd->skgbd', probs, value_float) / total[..., None]
        return jnp.transpose(summed, (3, 0, 1, 2, 4)).astype(jnp.bfloat16)
    mixed = lax.map(attend, query_blocks).reshape(LEN * SEQS, HEADS * HEAD_DIM)
    width = HEADS * HEAD_DIM // N_TP
    accum = jnp.zeros((LEN * SEQS, D), jnp.float32)
    for index in range(N_TP):
        part = jnp.dot(mixed[:, index * width:(index + 1) * width], out_weight[index * width:(index + 1) * width], preferred_element_type=jnp.float32)
        accum = accum + lax.optimization_barrier(part.astype(jnp.bfloat16)).astype(jnp.float32)
    attended = accum.astype(jnp.bfloat16).reshape(LEN, SEQS, D)
    token_float = moe_tokens.astype(jnp.float32)
    normed = (token_float * lax.rsqrt(lax.optimization_barrier(jnp.mean(token_float * token_float, axis=-1, keepdims=True)) + EPS) * moe_gain).astype(jnp.bfloat16)
    most = N_EP * N_TP * CAP
    unit_width = FF // N_TP

    def expert(carry, item):
        index, gate_weight, up_weight, down_weight = item
        chosen = routes == index
        weight = lax.optimization_barrier(jnp.sum(jnp.where(chosen, route_weight, 0.0), axis=1))
        live = jnp.any(chosen, axis=1)
        rows = jnp.nonzero(live, size=most, fill_value=0)[0].astype(jnp.int32)
        count = jnp.sum(live.astype(jnp.int32))
        valid = (jnp.arange(most, dtype=jnp.int32) < count).astype(jnp.float32)
        picked = normed[rows]
        gate = jnp.dot(picked, gate_weight, preferred_element_type=jnp.float32)
        up = jnp.dot(picked, up_weight, preferred_element_type=jnp.float32)
        hidden = (jax.nn.silu(gate) * up).astype(jnp.bfloat16)
        out = jnp.zeros((most, D), jnp.float32)
        for block_index in range(N_TP):
            part = jnp.dot(hidden[:, block_index * unit_width:(block_index + 1) * unit_width], down_weight[block_index * unit_width:(block_index + 1) * unit_width], preferred_element_type=jnp.float32)
            out = out + lax.optimization_barrier(part.astype(jnp.bfloat16)).astype(jnp.float32)
        expert_out = lax.optimization_barrier(out.astype(jnp.bfloat16)).astype(jnp.float32)
        contrib = expert_out * (weight[rows] * valid)[:, None]
        return (carry.at[rows].add(contrib), None)
    routed, _ = lax.scan(expert, jnp.zeros((TOKENS, D), jnp.float32), (jnp.arange(EXPERTS, dtype=jnp.int32), w_gate, w_up, w_down))
    return (attended, routed.astype(jnp.bfloat16))
```

```python
import functools
import math

import jax
import jax.numpy as jnp
from jax import lax
from jax.experimental import pallas as pl
from jax.experimental.pallas import tpu as pltpu
from jax.sharding import PartitionSpec as P

HEAD_DIM = 64
QUARTER = HEAD_DIM // 4
GRID_W = 64

EPS = 1e-06
THETA = 10000.0

MESH = pl.DeviceIdType.MESH


def exclusive_or(a, b, count):
    result = 0
    bit = 1
    while bit < count:
        result = result + (a // bit + b // bit) % 2 * bit
        bit *= 2
    return result


def turned(block, gain, cosine, sine):
    block = block.astype(jnp.float32)
    mean = jnp.mean(block * block, axis=0, keepdims=True)
    normed = block * lax.rsqrt(mean + EPS) * gain
    parts = []
    for axis in range(2):
        first = normed[2 * axis * QUARTER : (2 * axis + 1) * QUARTER]
        second = normed[(2 * axis + 1) * QUARTER : (2 * axis + 2) * QUARTER]
        c = cosine[axis * QUARTER : (axis + 1) * QUARTER]
        s = sine[axis * QUARTER : (axis + 1) * QUARTER]
        parts += [first * c - second * s, second * c + first * s]
    return jnp.concatenate(parts, axis=0).astype(jnp.bfloat16)


def fused_kernel(
    experts, capacity, tokens, moe_gain, routes, weights, queries, keys, values, q_gain, k_gain, cosine, sine,
    out_weight_hbm, w_gate_hbm, w_up_hbm, w_down_hbm, routed, att, *scratch
):
    (send, rows, part, pair, gone, seen, done, ret, packed, normed) = scratch[:10]
    (kv_all, q, prod, pair_att, gone_att, seen_att, accum, best, total, codes, combined) = scratch[10:21]
    (out_weight, w_gate, w_up, w_down, w_sem, own) = scratch[21:27]
    (a_send, a_recv, y_send, y_recv, l_send, l_recv, m_send, m_recv, k_send, k_recv, x_send, x_recv) = scratch[27:39]
    (f_send, f_recv, n_send, n_recv, c_send, c_recv, b_send, b_recv, o_send, o_recv) = scratch[39:]
    f32, bf16 = jnp.float32, jnp.bfloat16
    e, t = lax.axis_index("ep"), lax.axis_index("tp")
    low, high = t + 1 - 2 * (t % 2), (t + 2) % 4
    low_high = (low + 2) % 4
    half = experts // 2
    side = e + 1 - 2 * (e % 2)
    stride = packed.shape[0] // 4
    streams = kv_all.shape[1]
    positions = kv_all.shape[3]
    groups = q.shape[2] // positions
    tok_count = tokens.shape[0]

    def peer(k):
        return exclusive_or(e, k, experts)

    def remote(src, dst, s, r, device):
        return pltpu.make_async_remote_copy(
            src_ref=src, dst_ref=dst, send_sem=s, recv_sem=r, device_id=device, device_id_type=MESH
        )

    def kv_direct(m):
        return remote(kv_all.at[0], kv_all.at[2 * m], k_send.at[m], k_recv.at[m], (peer(2 * m), t))

    def kv_side(m):
        return remote(kv_all.at[2 * m], kv_all.at[2 * m + 1], x_send.at[m], x_recv.at[m], (side, t))

    def chunk(k):
        return remote(send.at[k], rows.at[t, k], a_send.at[k], a_recv.at[k], (peer(k), t))

    def across(k):
        block = rows.at[t, k]
        return remote(block, block, y_send.at[k], y_recv.at[k], (e, high))

    def beside(k):
        block = rows.at[t, k]
        return remote(block, block, l_send.at[k], l_recv.at[k], (e, low))

    def relay(k):
        block = rows.at[high, k]
        return remote(block, block, m_send.at[k], m_recv.at[k], (e, low))

    def pair_far(k):
        return remote(part.at[low_high, k], pair.at[1, k], f_send.at[k], f_recv.at[k], (e, low))

    def pair_near(k):
        return remote(part.at[low, k], pair.at[0, k], n_send.at[k], n_recv.at[k], (e, low))

    def over(k):
        return remote(gone.at[k], seen.at[k], c_send.at[k], c_recv.at[k], (e, high))

    def back(k):
        return remote(done.at[k], ret.at[k], b_send.at[k], b_recv.at[k], (peer(k), t))

    def other(i):
        if i < 2:
            return remote(prod.at[(low, low_high)[i]], pair_att.at[i], o_send.at[i], o_recv.at[i], (e, low))
        return remote(gone_att, seen_att, o_send.at[i], o_recv.at[i], (e, high))

    def own_copy(i):
        if i == 0:
            return pltpu.make_async_copy(send.at[0], rows.at[t, 0], own.at[0])
        return pltpu.make_async_copy(done.at[0], ret.at[0], own.at[1])

    def weight_copy(i):
        pairs = ((out_weight_hbm, out_weight), (w_gate_hbm, w_gate), (w_up_hbm, w_up), (w_down_hbm, w_down))
        return pltpu.make_async_copy(pairs[i][0], pairs[i][1], w_sem.at[i])

    def attend(j):
        for s in range(streams):
            key_block = kv_all[j, s, :HEAD_DIM]
            value_block = kv_all[j, s, HEAD_DIM:]
            scores = lax.dot_general(key_block, q[s], (((0,), (0,)), ((), ())), preferred_element_type=f32)
            old = best[s]
            new = jnp.maximum(old, jnp.max(scores, axis=0, keepdims=True))
            factor = jnp.exp(old - new)
            expo = jnp.exp(scores - new)
            best[s] = new
            total[s] = total[s] * factor + jnp.sum(expo, axis=0, keepdims=True)
            added = jnp.dot(value_block, expo.astype(bf16), preferred_element_type=f32)
            accum[s] = accum[s] * factor + added

    def project():
        quarter = positions // 4
        for s in range(streams):
            mixed = (accum[s] / total[s]).astype(bf16)
            stacked = jnp.concatenate([mixed[:, g * positions : (g + 1) * positions] for g in range(groups)], axis=0)
            product = lax.dot_general(stacked, out_weight[...], (((0,), (0,)), ((), ())), preferred_element_type=f32)
            product = product.astype(bf16)
            for b in range(4):
                prod[b, s * quarter : (s + 1) * quarter, :] = product[b * quarter : (b + 1) * quarter]

    def expert(k):
        for b in range(4):
            packed[b * stride : b * stride + capacity, :] = rows[b, k]
        data = packed[...]
        gate = jnp.dot(data, w_gate[...], preferred_element_type=f32)
        up = jnp.dot(data, w_up[...], preferred_element_type=f32)
        hidden = (gate * (1.0 / (1.0 + jnp.exp(-gate))) * up).astype(bf16)
        result = jnp.dot(hidden, w_down[...], preferred_element_type=f32).astype(bf16)
        for b in range(4):
            part[b, k] = result[b * stride : b * stride + capacity]

    def places(k):
        row = codes[pl.ds(peer(k), 1), :]
        slot = lax.broadcasted_iota(jnp.int32, (stride, tok_count), 0).astype(f32)
        return (slot == row).astype(f32)

    batch = min(experts, 4)

    def dispatch(g):
        table = jnp.concatenate([places(g * batch + i) for i in range(batch)], axis=0).astype(bf16)
        chosen = jnp.dot(table, normed[...], preferred_element_type=f32).astype(bf16)
        for i in range(batch):
            send[g * batch + i] = chosen[i * stride : i * stride + capacity]

    def send_batch(g):
        for i in range(batch):
            if i == 0:

                @pl.when(g > 0)
                def _():
                    chunk(g * batch).start()
            else:
                chunk(g * batch + i).start()

    def column(row):
        square = (tok_count, tok_count)
        diagonal = lax.broadcasted_iota(jnp.int32, square, 0) == lax.broadcasted_iota(jnp.int32, square, 1)
        return jnp.sum(jnp.where(diagonal, row, 0.0), axis=1, keepdims=True)

    def combine(k):
        if stride == capacity:
            data = ret[k]
        else:
            packed[:capacity, :] = ret[k]
            data = packed[:stride]
        table = places(k)
        picked = lax.dot_general(table.astype(bf16), data, (((0,), (0,)), ((), ())), preferred_element_type=f32)
        expert_id = peer(k)
        weight_row = jnp.zeros((1, tok_count), f32)
        for c in range(routes.shape[0]):
            weight_row = weight_row + jnp.where(routes[c : c + 1] == expert_id, weights[c : c + 1], 0.0)
        combined[...] += picked * column(weight_row)

    for i in range(4):
        weight_copy(i).start()
    barrier = pltpu.get_barrier_semaphore()
    partners = [(peer(k), t) for k in range(1, experts)] + [(e, low), (e, high)]
    for device in partners:
        pl.semaphore_signal(barrier, inc=1, device_id=device, device_id_type=MESH)

    for s in range(streams):
        kv_all[0, s, :HEAD_DIM] = turned(keys[s], k_gain[...], cosine[...], sine[...])
        kv_all[0, s, HEAD_DIM:] = values[s]

    if stride != capacity:
        packed[...] = jnp.zeros_like(packed)
    hits = jnp.zeros((experts, tok_count), f32)
    for c in range(routes.shape[0]):
        named = lax.broadcasted_iota(jnp.int32, (experts, tok_count), 0) == routes[c : c + 1]
        hits = hits + named.astype(f32)
    square = (tok_count, tok_count)
    earlier = lax.broadcasted_iota(jnp.int32, square, 0) < lax.broadcasted_iota(jnp.int32, square, 1)
    rank = jnp.dot(hits.astype(bf16), earlier.astype(f32).astype(bf16), preferred_element_type=f32)
    codes[...] = jnp.where(hits > 0.0, rank, -1.0)
    token_float = tokens[...].astype(f32)
    mean = jnp.mean(token_float * token_float, axis=-1, keepdims=True)
    normed[...] = (token_float * lax.rsqrt(mean + EPS) * moe_gain[...]).astype(bf16)

    pl.semaphore_wait(barrier, len(partners))

    lax.fori_loop(1, half, lambda m, c: (kv_direct(m).start(), c)[1], 0)
    kv_side(0).start()

    def dispatch_step(g, carry):
        @pl.when(g < experts // batch)
        def _():
            dispatch(g)

        @pl.when(g > 0)
        def _():
            send_batch(g - 1)

        @pl.when(g == experts // batch - 1)
        def _():
            for s in range(streams):
                for h in range(groups):
                    head = turned(queries[s, h * HEAD_DIM : (h + 1) * HEAD_DIM], q_gain[...], cosine[...], sine[...])
                    q[s, :, h * positions : (h + 1) * positions] = head * bf16(HEAD_DIM**-0.5)

        @pl.when(g == 1)
        def _():
            own_copy(0).start()

        return carry

    lax.fori_loop(0, experts // batch + 1, dispatch_step, 0)
    best[...] = jnp.full_like(best, -1e30)
    total[...] = jnp.zeros_like(total)
    accum[...] = jnp.zeros_like(accum)
    combined[...] = jnp.zeros_like(combined)
    own_copy(0).wait()
    across(0).start()
    beside(0).start()

    early = 2

    def attention_step(m, carry):
        attend(2 * m)

        @pl.when(m + 1 < half)
        def _():
            kv_direct(m + 1).wait_recv()
            kv_side(m + 1).start()

        kv_side(m).wait_recv()
        attend(2 * m + 1)

        @pl.when(m == half - 3)
        def _():
            chunk(1).wait_recv()
            across(1).start()
            beside(1).start()

        return carry

    lax.fori_loop(0, half, attention_step, 0)
    weight_copy(0).wait()
    project()
    for i in range(1, 4):
        weight_copy(i).wait()

    def step(k, carry):
        @pl.when((k >= early) & (k < experts))
        def _():
            chunk(k).wait_recv()
            across(k).start()
            beside(k).start()

        @pl.when((k >= 3) & (k < experts + 3))
        def _():
            pair_far(k - 3).start()
            pair_near(k - 3).start()

        @pl.when((k >= 5) & (k < experts + 5))
        def _():
            over(k - 5).start()

        @pl.when((k >= 8) & (k < experts + 7))
        def _():
            back(k - 7).start()

        @pl.when(k == 7)
        def _():
            own_copy(1).start()

        @pl.when(k == 1)
        def _():
            other(1).start()
            other(0).start()

        @pl.when((k >= 1) & (k < experts + 1))
        def _():
            across(k - 1).wait_recv()
            relay(k - 1).start()

        @pl.when(k == 3)
        def _():
            other(2).start()

        @pl.when((k >= 2) & (k < experts + 2))
        def _():
            beside(k - 2).wait_recv()
            relay(k - 2).wait_recv()
            expert(k - 2)

        @pl.when(k == 2)
        def _():
            other(1).wait_recv()
            gone_att[...] = (prod[high].astype(f32) + pair_att[1].astype(f32)).astype(bf16)

        @pl.when((k >= 4) & (k < experts + 4))
        def _():
            j = k - 4
            pair_far(j).wait_recv()
            gone[j] = (part[high, j].astype(f32) + pair[1, j].astype(f32)).astype(bf16)

        @pl.when((k >= 6) & (k < experts + 6))
        def _():
            j = k - 6
            pair_near(j).wait_recv()
            over(j).wait_recv()
            done[j] = (part[t, j].astype(f32) + pair[0, j].astype(f32) + seen[j].astype(f32)).astype(bf16)

        @pl.when((k >= 10) & (k < experts + 9))
        def _():
            back(k - 9).wait_recv()
            combine(k - 9)

        @pl.when(k == 9)
        def _():
            own_copy(1).wait()
            combine(0)

        @pl.when(k == experts + 1)
        def _():
            other(0).wait_recv()
            other(2).wait_recv()
            att[...] = (prod[t].astype(f32) + pair_att[0].astype(f32) + seen_att[...].astype(f32)).astype(bf16)

        return carry

    lax.fori_loop(0, experts + 9, step, 0)
    routed[...] = combined[...].astype(bf16)

    def finish(k, carry):
        across(k).wait_send()
        beside(k).wait_send()
        relay(k).wait_send()
        pair_far(k).wait_send()
        pair_near(k).wait_send()
        over(k).wait_send()

        @pl.when(k >= 1)
        def _():
            chunk(k).wait_send()
            back(k).wait_send()

        @pl.when(k < half)
        def _():
            kv_side(k).wait_send()

        @pl.when((k >= 1) & (k < half))
        def _():
            kv_direct(k).wait_send()

        return carry

    lax.fori_loop(0, experts, finish, 0)
    for i in range(3):
        other(i).wait_send()


def fused(experts, capacity, tokens, moe_gain, routes, weights, queries, keys, *rest):
    values, q_gain, k_gain, cosine, sine, out_weight, w_gate, w_up, w_down = rest
    like = tokens.dtype
    f32 = jnp.float32
    sem = pltpu.SemaphoreType.DMA((experts,))
    tok_count, features = tokens.shape
    streams, _, positions = keys.shape
    query_lanes = queries.shape[1] // HEAD_DIM * positions
    att = (positions // 4 * streams, features)
    stride = -(-capacity // 16) * 16
    block = (experts, capacity, features)
    shapes = [
        (block, like),
        ((4,) + block, like),
        ((4,) + block, like),
        ((2,) + block, like),
        (block, like),
        (block, like),
        (block, like),
        (block, like),
        ((4 * stride, features), like),
        (tokens.shape, like),
        ((experts, streams, 2 * HEAD_DIM, positions), like),
        ((streams, HEAD_DIM, query_lanes), like),
        ((4,) + att, like),
        ((2,) + att, like),
        (att, like),
        (att, like),
        ((streams, HEAD_DIM, query_lanes), f32),
        ((streams, 1, query_lanes), f32),
        ((streams, 1, query_lanes), f32),
        ((experts, tok_count), f32),
        (tokens.shape, f32),
        (out_weight.shape, like),
        (w_gate.shape, like),
        (w_up.shape, like),
        (w_down.shape, like),
    ]
    vmem = pl.BlockSpec(memory_space=pltpu.VMEM)
    hbm = pl.BlockSpec(memory_space=pl.ANY)
    return pl.pallas_call(
        functools.partial(fused_kernel, experts, capacity),
        out_shape=(jax.ShapeDtypeStruct(tokens.shape, like), jax.ShapeDtypeStruct(att, like)),
        in_specs=[vmem] * 11 + [hbm] * 4,
        out_specs=(vmem, vmem),
        scratch_shapes=[pltpu.VMEM(shape, dtype) for shape, dtype in shapes]
        + [pltpu.SemaphoreType.DMA((4,)), pltpu.SemaphoreType.DMA((2,))]
        + [sem] * 20
        + [pltpu.SemaphoreType.DMA((3,))] * 2,
        name="fused",
        compiler_params=pltpu.CompilerParams(
            collective_id=1, has_side_effects=True, vmem_limit_bytes=62 * 2**20
        ),
    )(tokens, moe_gain, routes, weights, queries, keys, values, q_gain, k_gain, cosine, sine,
      out_weight, w_gate, w_up, w_down)


def per_device(
    queries,
    keys,
    values,
    query_gain,
    key_gain,
    out_weight,
    moe_tokens,
    moe_gain,
    routes,
    route_weight,
    w_gate,
    w_up,
    w_down,
):
    pos_count, seq_count = queries.shape[:2]
    positions = lax.axis_index("ep") * pos_count + jnp.arange(pos_count, dtype=jnp.int32)
    inverse = THETA ** (-jnp.arange(QUARTER, dtype=jnp.float32) / QUARTER)
    grid_row = (positions // GRID_W).astype(jnp.float32)
    grid_col = (positions % GRID_W).astype(jnp.float32)
    angles = jnp.concatenate([inverse[:, None] * grid_row, inverse[:, None] * grid_col], axis=0)
    kv_local = keys.shape[2] // HEAD_DIM
    streams = seq_count * kv_local
    experts = lax.axis_size("ep")
    capacity = max(2, (3 * moe_tokens.shape[0] * routes.shape[1] + 2 * experts - 1) // (2 * experts))

    def by_feature(data):
        return jnp.transpose(data, (1, 2, 0)).reshape(streams, -1, pos_count)

    def wide(gain):
        return jnp.broadcast_to(gain[:, None], (HEAD_DIM, pos_count))

    routed, attended = fused(
        experts,
        capacity,
        moe_tokens,
        moe_gain[None, :],
        routes.T,
        route_weight.T,
        by_feature(queries),
        by_feature(keys),
        by_feature(values),
        wide(query_gain),
        wide(key_gain),
        jnp.cos(angles),
        jnp.sin(angles),
        out_weight,
        w_gate[0],
        w_up[0],
        w_down[0],
    )
    quarter = pos_count // lax.axis_size("tp")
    attended = jnp.transpose(attended.reshape(seq_count, quarter, -1), (1, 0, 2))
    return (attended, routed)


def solution(mesh):
    in_specs = (
        P("ep", None, "tp"),
        P("ep", None, "tp"),
        P("ep", None, "tp"),
        P(),
        P(),
        P("tp", None),
        P(("ep", "tp"), None),
        P(),
        P(("ep", "tp"), None),
        P(("ep", "tp"), None),
        P("ep", None, "tp"),
        P("ep", None, "tp"),
        P("ep", "tp", None),
    )
    out_specs = (P(("ep", "tp"), None, None), P(("ep", "tp"), None))
    return jax.shard_map(
        per_device, mesh=mesh, in_specs=in_specs, out_specs=out_specs, check_vma=False
    )
```

```python
import functools
import math

import jax
import jax.numpy as jnp
from jax import lax
from jax.experimental import pallas as pl
from jax.experimental.pallas import tpu as pltpu
from jax.sharding import PartitionSpec as P

HEAD_DIM = 64
QUARTER = HEAD_DIM // 4
GRID_W = 64

EPS = 1e-06
THETA = 10000.0

MESH = pl.DeviceIdType.MESH


def exclusive_or(a, b, count):
    result = 0
    bit = 1
    while bit < count:
        result = result + (a // bit + b // bit) % 2 * bit
        bit *= 2
    return result


def pick(place, special, rest):
    for where, value in special:
        rest = jnp.where(place == where, value, rest)
    return rest


def in_order(place):
    return pick(place, ((3, 4), (4, 5), (5, 3)), place)


def out_order(place, count):
    return pick(place, ((0, 4), (1, 5), (2, 1), (count - 3, 2), (count - 2, 3), (count - 1, 0)), place + 3)


def turned(block, gain, cosine, sine):
    block = block.astype(jnp.float32)
    mean = jnp.mean(block * block, axis=0, keepdims=True)
    normed = block * lax.rsqrt(mean + EPS) * gain
    parts = []
    for axis in range(2):
        first = normed[2 * axis * QUARTER : (2 * axis + 1) * QUARTER]
        second = normed[(2 * axis + 1) * QUARTER : (2 * axis + 2) * QUARTER]
        c = cosine[axis * QUARTER : (axis + 1) * QUARTER]
        s = sine[axis * QUARTER : (axis + 1) * QUARTER]
        parts += [first * c - second * s, second * c + first * s]
    return jnp.concatenate(parts, axis=0).astype(jnp.bfloat16)


def fused_kernel(
    experts, capacity, tokens, moe_gain, routes, weights, queries, keys, values, q_gain, k_gain, cosine, sine,
    out_weight_hbm, w_gate_hbm, w_up_hbm, w_down_hbm, routed, att, *scratch
):
    (send, rows, part, pair, gone, seen, done, ret, packed, normed) = scratch[:10]
    (kv_all, q, prod, pair_att, gone_att, seen_att, accum, best, total, codes, combined) = scratch[10:21]
    (out_weight, w_gate, w_up, w_down, w_sem, own) = scratch[21:27]
    (a_send, a_recv, y_send, y_recv, l_send, l_recv, m_send, m_recv, k_send, k_recv, x_send, x_recv) = scratch[27:39]
    (f_send, f_recv, n_send, n_recv, c_send, c_recv, b_send, b_recv, o_send, o_recv) = scratch[39:]
    f32, bf16 = jnp.float32, jnp.bfloat16
    e, t = lax.axis_index("ep"), lax.axis_index("tp")
    low, high = t + 1 - 2 * (t % 2), (t + 2) % 4
    low_high = (low + 2) % 4
    half = experts // 2
    side = e + 1 - 2 * (e % 2)
    stride = packed.shape[0] // 4
    streams = kv_all.shape[1]
    positions = kv_all.shape[3]
    groups = q.shape[2] // positions
    tok_count = tokens.shape[0]

    def peer(k):
        return exclusive_or(e, k, experts)

    def remote(src, dst, s, r, device):
        return pltpu.make_async_remote_copy(
            src_ref=src, dst_ref=dst, send_sem=s, recv_sem=r, device_id=device, device_id_type=MESH
        )

    def kv_direct(m):
        return remote(kv_all.at[0], kv_all.at[2 * m], k_send.at[m], k_recv.at[m], (peer(2 * m), t))

    def kv_side(m):
        return remote(kv_all.at[2 * m], kv_all.at[2 * m + 1], x_send.at[m], x_recv.at[m], (side, t))

    def chunk(k):
        return remote(send.at[k], rows.at[t, k], a_send.at[k], a_recv.at[k], (peer(k), t))

    def across(k):
        block = rows.at[t, k]
        return remote(block, block, y_send.at[k], y_recv.at[k], (e, high))

    def beside(k):
        block = rows.at[t, k]
        return remote(block, block, l_send.at[k], l_recv.at[k], (e, low))

    def relay(k):
        block = rows.at[high, k]
        return remote(block, block, m_send.at[k], m_recv.at[k], (e, low))

    def pair_far(k):
        return remote(part.at[low_high, k], pair.at[1, k], f_send.at[k], f_recv.at[k], (e, low))

    def pair_near(k):
        return remote(part.at[low, k], pair.at[0, k], n_send.at[k], n_recv.at[k], (e, low))

    def over(k):
        return remote(gone.at[k], seen.at[k], c_send.at[k], c_recv.at[k], (e, high))

    def back(k):
        return remote(done.at[k], ret.at[k], b_send.at[k], b_recv.at[k], (peer(k), t))

    def other(i):
        if i < 2:
            return remote(prod.at[(low, low_high)[i]], pair_att.at[i], o_send.at[i], o_recv.at[i], (e, low))
        return remote(gone_att, seen_att, o_send.at[i], o_recv.at[i], (e, high))

    def own_copy(i):
        if i == 0:
            return pltpu.make_async_copy(send.at[0], rows.at[t, 0], own.at[0])
        return pltpu.make_async_copy(done.at[0], ret.at[0], own.at[1])

    def weight_copy(i):
        pairs = ((out_weight_hbm, out_weight), (w_gate_hbm, w_gate), (w_up_hbm, w_up), (w_down_hbm, w_down))
        return pltpu.make_async_copy(pairs[i][0], pairs[i][1], w_sem.at[i])

    def attend(j):
        for s in range(streams):
            key_block = kv_all[j, s, :HEAD_DIM]
            value_block = kv_all[j, s, HEAD_DIM:]
            scores = lax.dot_general(key_block, q[s], (((0,), (0,)), ((), ())), preferred_element_type=f32)
            old = best[s]
            new = jnp.maximum(old, jnp.max(scores, axis=0, keepdims=True))
            factor = jnp.exp(old - new)
            expo = jnp.exp(scores - new)
            best[s] = new
            total[s] = total[s] * factor + jnp.sum(expo, axis=0, keepdims=True)
            added = jnp.dot(value_block, expo.astype(bf16), preferred_element_type=f32)
            accum[s] = accum[s] * factor + added

    def project():
        quarter = positions // 4
        for s in range(streams):
            mixed = (accum[s] / total[s]).astype(bf16)
            stacked = jnp.concatenate([mixed[:, g * positions : (g + 1) * positions] for g in range(groups)], axis=0)
            product = lax.dot_general(stacked, out_weight[...], (((0,), (0,)), ((), ())), preferred_element_type=f32)
            product = product.astype(bf16)
            for b in range(4):
                prod[b, s * quarter : (s + 1) * quarter, :] = product[b * quarter : (b + 1) * quarter]

    def expert(k):
        for b in range(4):
            packed[b * stride : b * stride + capacity, :] = rows[b, k]
        data = packed[...]
        gate = jnp.dot(data, w_gate[...], preferred_element_type=f32)
        up = jnp.dot(data, w_up[...], preferred_element_type=f32)
        hidden = (gate * (1.0 / (1.0 + jnp.exp(-gate))) * up).astype(bf16)
        result = jnp.dot(hidden, w_down[...], preferred_element_type=f32).astype(bf16)
        for b in range(4):
            part[b, k] = result[b * stride : b * stride + capacity]

    def places(k):
        row = codes[pl.ds(peer(k), 1), :]
        slot = lax.broadcasted_iota(jnp.int32, (stride, tok_count), 0).astype(f32)
        return (slot == row).astype(f32)

    batch = min(experts, 4)
    kv_at, attend_at = 5, 9

    def dispatch(g):
        table = jnp.concatenate([places(g * batch + i) for i in range(batch)], axis=0).astype(bf16)
        chosen = jnp.dot(table, normed[...], preferred_element_type=f32).astype(bf16)
        for i in range(batch):
            send[g * batch + i] = chosen[i * stride : i * stride + capacity]

    def column(row):
        square = (tok_count, tok_count)
        diagonal = lax.broadcasted_iota(jnp.int32, square, 0) == lax.broadcasted_iota(jnp.int32, square, 1)
        return jnp.sum(jnp.where(diagonal, row, 0.0), axis=1, keepdims=True)

    def combine(k):
        if stride == capacity:
            data = ret[k]
        else:
            packed[:capacity, :] = ret[k]
            data = packed[:stride]
        table = places(k)
        picked = lax.dot_general(table.astype(bf16), data, (((0,), (0,)), ((), ())), preferred_element_type=f32)
        expert_id = peer(k)
        weight_row = jnp.zeros((1, tok_count), f32)
        for c in range(routes.shape[0]):
            weight_row = weight_row + jnp.where(routes[c : c + 1] == expert_id, weights[c : c + 1], 0.0)
        combined[...] += picked * column(weight_row)

    for i in range(4):
        weight_copy(i).start()
    barrier = pltpu.get_barrier_semaphore()
    partners = [(peer(k), t) for k in range(1, experts)] + [(e, low), (e, high)]
    for device in partners:
        pl.semaphore_signal(barrier, inc=1, device_id=device, device_id_type=MESH)

    for s in range(streams):
        kv_all[0, s, :HEAD_DIM] = turned(keys[s], k_gain[...], cosine[...], sine[...])
        kv_all[0, s, HEAD_DIM:] = values[s]

    if stride != capacity:
        packed[...] = jnp.zeros_like(packed)
    hits = jnp.zeros((experts, tok_count), f32)
    for c in range(routes.shape[0]):
        named = lax.broadcasted_iota(jnp.int32, (experts, tok_count), 0) == routes[c : c + 1]
        hits = hits + named.astype(f32)
    square = (tok_count, tok_count)
    earlier = lax.broadcasted_iota(jnp.int32, square, 0) < lax.broadcasted_iota(jnp.int32, square, 1)
    rank = jnp.dot(hits.astype(bf16), earlier.astype(f32).astype(bf16), preferred_element_type=f32)
    codes[...] = jnp.where(hits > 0.0, rank, -1.0)
    token_float = tokens[...].astype(f32)
    mean = jnp.mean(token_float * token_float, axis=-1, keepdims=True)
    normed[...] = (token_float * lax.rsqrt(mean + EPS) * moe_gain[...]).astype(bf16)

    pl.semaphore_wait(barrier, len(partners))

    lax.fori_loop(0, experts // batch, lambda g, c: (dispatch(g), c)[1], 0)
    for s in range(streams):
        for h in range(groups):
            head = turned(queries[s, h * HEAD_DIM : (h + 1) * HEAD_DIM], q_gain[...], cosine[...], sine[...])
            q[s, :, h * positions : (h + 1) * positions] = head * bf16(HEAD_DIM**-0.5)
    own_copy(0).start()
    for k in (1, 2, 4, 5):
        chunk(k).start()
    best[...] = jnp.full_like(best, -1e30)
    total[...] = jnp.zeros_like(total)
    accum[...] = jnp.zeros_like(accum)
    combined[...] = jnp.zeros_like(combined)
    own_copy(0).wait()
    for i in range(4):
        weight_copy(i).wait()

    def step(i, carry):
        def within(least, most):
            return pl.when((i >= least) & (i < most))

        def when_out(delay):
            return within(delay, experts + delay)

        def out(delay):
            return out_order(i - delay, experts)

        @within(0, experts)
        def _():
            k = in_order(i)

            @pl.when(i > 0)
            def _():
                chunk(k).wait_recv()

            across(k).start()
            beside(k).start()

            @pl.when(k == 2)
            def _():
                chunk(3).start()

            @pl.when((k >= 4) & (k + 2 < experts))
            def _():
                chunk(k + 2).start()

        @within(kv_at, kv_at + 1)
        def _():
            kv_side(0).start()
            lax.fori_loop(1, half, lambda m, c: (kv_direct(m).start(), c)[1], 0)

        @within(1, experts + 1)
        def _():
            k = in_order(i - 1)
            across(k).wait_recv()
            relay(k).start()

        @when_out(5)
        def _():
            j = out(5)
            beside(j).wait_recv()
            relay(j).wait_recv()
            expert(j)

        @when_out(6)
        def _():
            j = out(6)
            pair_far(j).wait_recv()
            gone[j] = (part[high, j].astype(f32) + pair[1, j].astype(f32)).astype(bf16)

        @within(attend_at + half + 1, attend_at + half + 2)
        def _():
            other(1).wait_recv()
            gone_att[...] = (prod[high].astype(f32) + pair_att[1].astype(f32)).astype(bf16)

        @when_out(8)
        def _():
            j = out(8)
            pair_near(j).wait_recv()
            over(j).wait_recv()
            done[j] = (part[t, j].astype(f32) + pair[0, j].astype(f32) + seen[j].astype(f32)).astype(bf16)

        @when_out(5)
        def _():
            pair_far(out(5)).start()
            pair_near(out(5)).start()

        @when_out(6)
        def _():
            over(out(6)).start()

        @within(8, experts + 7)
        def _():
            back(out(8)).start()

        @within(experts + 7, experts + 8)
        def _():
            own_copy(1).start()

        @within(attend_at + half + 1, attend_at + half + 2)
        def _():
            other(2).start()

        @within(attend_at - 1, attend_at + half - 2)
        def _():
            m = i - attend_at + 2
            kv_direct(m).wait_recv()
            kv_side(m).start()

        @within(attend_at, attend_at + half)
        def _():
            m = i - attend_at
            attend(2 * m)
            kv_side(m).wait_recv()
            attend(2 * m + 1)

        @within(attend_at + half, attend_at + half + 1)
        def _():
            project()
            other(1).start()
            other(0).start()

        return carry

    lax.fori_loop(0, experts + 8, step, 0)

    def gather(k, carry):
        @pl.when(k == 0)
        def _():
            own_copy(1).wait()

        @pl.when(k > 0)
        def _():
            back(k).wait_recv()

        @pl.when(k == 3)
        def _():
            other(0).wait_recv()
            other(2).wait_recv()
            att[...] = (prod[t].astype(f32) + pair_att[0].astype(f32) + seen_att[...].astype(f32)).astype(bf16)

        combine(k)
        return carry

    lax.fori_loop(0, experts, gather, 0)
    routed[...] = combined[...].astype(bf16)

    def finish(k, carry):
        across(k).wait_send()
        beside(k).wait_send()
        relay(k).wait_send()
        pair_far(k).wait_send()
        pair_near(k).wait_send()
        over(k).wait_send()

        @pl.when(k >= 1)
        def _():
            back(k).wait_send()
            chunk(k).wait_send()

        @pl.when(k < half)
        def _():
            kv_side(k).wait_send()

        @pl.when((k >= 1) & (k < half))
        def _():
            kv_direct(k).wait_send()

        return carry

    lax.fori_loop(0, experts, finish, 0)
    for i in range(3):
        other(i).wait_send()


def fused(experts, capacity, tokens, moe_gain, routes, weights, queries, keys, *rest):
    values, q_gain, k_gain, cosine, sine, out_weight, w_gate, w_up, w_down = rest
    like = tokens.dtype
    f32 = jnp.float32
    sem = pltpu.SemaphoreType.DMA((experts,))
    tok_count, features = tokens.shape
    streams, _, positions = keys.shape
    query_lanes = queries.shape[1] // HEAD_DIM * positions
    att = (positions // 4 * streams, features)
    stride = -(-capacity // 16) * 16
    block = (experts, capacity, features)
    shapes = [
        (block, like),
        ((4,) + block, like),
        ((4,) + block, like),
        ((2,) + block, like),
        (block, like),
        (block, like),
        (block, like),
        (block, like),
        ((4 * stride, features), like),
        (tokens.shape, like),
        ((experts, streams, 2 * HEAD_DIM, positions), like),
        ((streams, HEAD_DIM, query_lanes), like),
        ((4,) + att, like),
        ((2,) + att, like),
        (att, like),
        (att, like),
        ((streams, HEAD_DIM, query_lanes), f32),
        ((streams, 1, query_lanes), f32),
        ((streams, 1, query_lanes), f32),
        ((experts, tok_count), f32),
        (tokens.shape, f32),
        (out_weight.shape, like),
        (w_gate.shape, like),
        (w_up.shape, like),
        (w_down.shape, like),
    ]
    vmem = pl.BlockSpec(memory_space=pltpu.VMEM)
    hbm = pl.BlockSpec(memory_space=pl.ANY)
    return pl.pallas_call(
        functools.partial(fused_kernel, experts, capacity),
        out_shape=(jax.ShapeDtypeStruct(tokens.shape, like), jax.ShapeDtypeStruct(att, like)),
        in_specs=[vmem] * 11 + [hbm] * 4,
        out_specs=(vmem, vmem),
        scratch_shapes=[pltpu.VMEM(shape, dtype) for shape, dtype in shapes]
        + [pltpu.SemaphoreType.DMA((4,)), pltpu.SemaphoreType.DMA((2,))]
        + [sem] * 20
        + [pltpu.SemaphoreType.DMA((3,))] * 2,
        name="fused",
        compiler_params=pltpu.CompilerParams(
            collective_id=1, has_side_effects=True, vmem_limit_bytes=62 * 2**20
        ),
    )(tokens, moe_gain, routes, weights, queries, keys, values, q_gain, k_gain, cosine, sine,
      out_weight, w_gate, w_up, w_down)


def per_device(
    queries,
    keys,
    values,
    query_gain,
    key_gain,
    out_weight,
    moe_tokens,
    moe_gain,
    routes,
    route_weight,
    w_gate,
    w_up,
    w_down,
):
    pos_count, seq_count = queries.shape[:2]
    positions = lax.axis_index("ep") * pos_count + jnp.arange(pos_count, dtype=jnp.int32)
    inverse = THETA ** (-jnp.arange(QUARTER, dtype=jnp.float32) / QUARTER)
    grid_row = (positions // GRID_W).astype(jnp.float32)
    grid_col = (positions % GRID_W).astype(jnp.float32)
    angles = jnp.concatenate([inverse[:, None] * grid_row, inverse[:, None] * grid_col], axis=0)
    kv_local = keys.shape[2] // HEAD_DIM
    streams = seq_count * kv_local
    experts = lax.axis_size("ep")
    capacity = max(2, (3 * moe_tokens.shape[0] * routes.shape[1] + 2 * experts - 1) // (2 * experts))

    def by_feature(data):
        return jnp.transpose(data, (1, 2, 0)).reshape(streams, -1, pos_count)

    def wide(gain):
        return jnp.broadcast_to(gain[:, None], (HEAD_DIM, pos_count))

    routed, attended = fused(
        experts,
        capacity,
        moe_tokens,
        moe_gain[None, :],
        routes.T,
        route_weight.T,
        by_feature(queries),
        by_feature(keys),
        by_feature(values),
        wide(query_gain),
        wide(key_gain),
        jnp.cos(angles),
        jnp.sin(angles),
        out_weight,
        w_gate[0],
        w_up[0],
        w_down[0],
    )
    quarter = pos_count // lax.axis_size("tp")
    attended = jnp.transpose(attended.reshape(seq_count, quarter, -1), (1, 0, 2))
    return (attended, routed)


def solution(mesh):
    in_specs = (
        P("ep", None, "tp"),
        P("ep", None, "tp"),
        P("ep", None, "tp"),
        P(),
        P(),
        P("tp", None),
        P(("ep", "tp"), None),
        P(),
        P(("ep", "tp"), None),
        P(("ep", "tp"), None),
        P("ep", None, "tp"),
        P("ep", None, "tp"),
        P("ep", "tp", None),
    )
    out_specs = (P(("ep", "tp"), None, None), P(("ep", "tp"), None))
    return jax.shard_map(
        per_device, mesh=mesh, in_specs=in_specs, out_specs=out_specs, check_vma=False
    )
```

```python
import functools
import math

import jax
import jax.numpy as jnp
from jax import lax
from jax.experimental import pallas as pl
from jax.experimental.pallas import tpu as pltpu
from jax.sharding import PartitionSpec as P

HEAD_DIM = 64
QUARTER = HEAD_DIM // 4
GRID_W = 64

EPS = 1e-06
THETA = 10000.0

MESH = pl.DeviceIdType.MESH


def exclusive_or(a, b, count):
    result = 0
    bit = 1
    while bit < count:
        result = result + (a // bit + b // bit) % 2 * bit
        bit *= 2
    return result


RANKS = "RSTLXDGPOQUBKVACJHI"


def schedule(experts, near):
    half = experts // 2
    far = list(range(near, experts))
    if near == 4 and experts == 8:
        listed = (
            "R1 K0 S5 T0", "R4 S6 Q0 U1", "X0 P0 G0 L4", "O0 V1 R5 S7", "V2 X4 P4 L1", "G4 O4 L5 X1",
            "P1 A0 R6 S2", "U2 X5 P5 G5", "O5 D4 B4 V3", "A1 L6 G1 O1", "R7 S3 U3 X6", "P6 D5 B5 G6",
            "O6 R2 L2 X2", "P2 G2 O2 L7", "X7 P7 A2 G7", "O7 D6 B6 R3", "L3 X3 P3 A3", "G3 O3 D7 B7",
            "J0 D1 B1 H0", "I0 D2 B2 C4", "C5 D0 B0 D3", "B3 C6 C0 C1", "C7 C2 C3",
        )
        return [(word[0], int(word[1:])) for word in " ".join(listed).split()]
    program = []
    for i in range(experts + 5):
        stages = (("R", 0), ("S", -2), ("L", 1), ("X", 2), ("D", 5), ("G", 3), ("P", 2), ("O", 3), ("B", 5))
        for name, delay in stages:
            if 0 <= i - delay < experts:
                program.append((name, i - delay))
    program.append(("K", 0))
    program += [("V", m) for m in range(1, half)] + [("A", m) for m in range(half)]
    return program + [("J", 0), ("H", 0), ("I", 0)] + [("C", k) for k in range(experts)]


def in_slots(program):
    tables, slot, last = {name: [] for name in RANKS}, 0, -1
    for name, number in program:
        rank = RANKS.index(name)
        if rank <= last:
            slot += 1
        last = rank
        tables[name].append((slot, number))
    return tables, slot + 1


def turned(block, gain, cosine, sine):
    block = block.astype(jnp.float32)
    mean = jnp.mean(block * block, axis=0, keepdims=True)
    normed = block * lax.rsqrt(mean + EPS) * gain
    parts = []
    for axis in range(2):
        first = normed[2 * axis * QUARTER : (2 * axis + 1) * QUARTER]
        second = normed[(2 * axis + 1) * QUARTER : (2 * axis + 2) * QUARTER]
        c = cosine[axis * QUARTER : (axis + 1) * QUARTER]
        s = sine[axis * QUARTER : (axis + 1) * QUARTER]
        parts += [first * c - second * s, second * c + first * s]
    return jnp.concatenate(parts, axis=0).astype(jnp.bfloat16)


def fused_kernel(
    experts, capacity, tokens, moe_gain, routes, weights, queries, keys, values, q_gain, k_gain, cosine, sine,
    out_weight_hbm, w_gate_hbm, w_up_hbm, w_down_hbm, routed, att, *scratch
):
    (send, rows, part, pair, gone, seen, done, ret, packed, normed) = scratch[:10]
    (kv_all, q, prod, pair_att, gone_att, seen_att, accum, best, total, codes, combined) = scratch[10:21]
    (out_weight, w_gate, w_up, w_down, passed, normed_high, codes_high, w_sem, own) = scratch[21:30]
    (a_send, a_recv, y_send, y_recv, l_send, l_recv, m_send, m_recv, k_send, k_recv, x_send, x_recv) = scratch[30:42]
    (f_send, f_recv, n_send, n_recv, c_send, c_recv, b_send, b_recv, o_send, o_recv) = scratch[42:52]
    (p_send, p_recv, t_send, t_recv) = scratch[52:]
    f32, bf16 = jnp.float32, jnp.bfloat16
    e, t = lax.axis_index("ep"), lax.axis_index("tp")
    low, high = t + 1 - 2 * (t % 2), (t + 2) % 4
    low_high = (low + 2) % 4
    half = experts // 2
    side = e + 1 - 2 * (e % 2)
    stride = packed.shape[0] // 4
    streams = kv_all.shape[1]
    positions = kv_all.shape[3]
    groups = q.shape[2] // positions
    tok_count = tokens.shape[0]

    def peer(k):
        return exclusive_or(e, k, experts)

    def remote(src, dst, s, r, device):
        return pltpu.make_async_remote_copy(
            src_ref=src, dst_ref=dst, send_sem=s, recv_sem=r, device_id=device, device_id_type=MESH
        )

    def kv_direct(m):
        return remote(kv_all.at[0], kv_all.at[2 * m], k_send.at[m], k_recv.at[m], (peer(2 * m), t))

    def kv_onward(m):
        return remote(kv_all.at[half], kv_all.at[2 * m], k_send.at[m], k_recv.at[m], (peer(2 * m - half), t))

    def kv_side(m):
        return remote(kv_all.at[2 * m], kv_all.at[2 * m + 1], x_send.at[m], x_recv.at[m], (side, t))

    def chunk(k):
        return remote(send.at[k], rows.at[t, k], a_send.at[k], a_recv.at[k], (peer(k), t))

    def passed_chunk(k):
        return remote(passed.at[k], rows.at[high, k], p_send.at[k], p_recv.at[k], (peer(k), t))

    def whole_block(i):
        src, dst = ((normed, normed_high), (codes, codes_high))[i]
        return remote(src, dst, t_send.at[i], t_recv.at[i], (e, high))

    def across(k):
        block = rows.at[t, k]
        return remote(block, block, y_send.at[k], y_recv.at[k], (e, high))

    def beside(k):
        block = rows.at[t, k]
        return remote(block, block, l_send.at[k], l_recv.at[k], (e, low))

    def relay(k):
        block = rows.at[high, k]
        return remote(block, block, m_send.at[k], m_recv.at[k], (e, low))

    def pair_far(k):
        return remote(part.at[low_high, k], pair.at[1, k], f_send.at[k], f_recv.at[k], (e, low))

    def pair_near(k):
        return remote(part.at[low, k], pair.at[0, k], n_send.at[k], n_recv.at[k], (e, low))

    def over(k):
        return remote(gone.at[k], seen.at[k], c_send.at[k], c_recv.at[k], (e, high))

    def back(k):
        return remote(done.at[k], ret.at[k], b_send.at[k], b_recv.at[k], (peer(k), t))

    def other(i):
        if i < 2:
            return remote(prod.at[(low, low_high)[i]], pair_att.at[i], o_send.at[i], o_recv.at[i], (e, low))
        return remote(gone_att, seen_att, o_send.at[i], o_recv.at[i], (e, high))

    def own_copy(i):
        if i == 0:
            return pltpu.make_async_copy(send.at[0], rows.at[t, 0], own.at[0])
        return pltpu.make_async_copy(done.at[0], ret.at[0], own.at[1])

    def weight_copy(i):
        pairs = ((out_weight_hbm, out_weight), (w_gate_hbm, w_gate), (w_up_hbm, w_up), (w_down_hbm, w_down))
        return pltpu.make_async_copy(pairs[i][0], pairs[i][1], w_sem.at[i])

    def attend(j):
        for s in range(streams):
            key_block = kv_all[j, s, :HEAD_DIM]
            value_block = kv_all[j, s, HEAD_DIM:]
            scores = lax.dot_general(key_block, q[s], (((0,), (0,)), ((), ())), preferred_element_type=f32)
            old = best[s]
            new = jnp.maximum(old, jnp.max(scores, axis=0, keepdims=True))
            factor = jnp.exp(old - new)
            expo = jnp.exp(scores - new)
            best[s] = new
            total[s] = total[s] * factor + jnp.sum(expo, axis=0, keepdims=True)
            added = jnp.dot(value_block, expo.astype(bf16), preferred_element_type=f32)
            accum[s] = accum[s] * factor + added

    def project():
        quarter = positions // 4
        for s in range(streams):
            mixed = (accum[s] / total[s]).astype(bf16)
            stacked = jnp.concatenate([mixed[:, g * positions : (g + 1) * positions] for g in range(groups)], axis=0)
            product = lax.dot_general(stacked, out_weight[...], (((0,), (0,)), ((), ())), preferred_element_type=f32)
            product = product.astype(bf16)
            for b in range(4):
                prod[b, s * quarter : (s + 1) * quarter, :] = product[b * quarter : (b + 1) * quarter]

    def expert(k):
        for b in range(4):
            packed[b * stride : b * stride + capacity, :] = rows[b, k]
        data = packed[...]
        gate = jnp.dot(data, w_gate[...], preferred_element_type=f32)
        up = jnp.dot(data, w_up[...], preferred_element_type=f32)
        hidden = (gate * (1.0 / (1.0 + jnp.exp(-gate))) * up).astype(bf16)
        result = jnp.dot(hidden, w_down[...], preferred_element_type=f32).astype(bf16)
        for b in range(4):
            part[b, k] = result[b * stride : b * stride + capacity]

    def places(k, table=codes):
        row = table[pl.ds(peer(k), 1), :]
        slot = lax.broadcasted_iota(jnp.int32, (stride, tok_count), 0).astype(f32)
        return (slot == row).astype(f32)

    batch = min(experts, 4)
    near = 4 if experts == 8 and 4 * capacity > tok_count else 0
    far = experts - near

    def dispatch(g):
        table = jnp.concatenate([places(g * batch + i) for i in range(batch)], axis=0).astype(bf16)
        chosen = jnp.dot(table, normed[...], preferred_element_type=f32).astype(bf16)
        for i in range(batch):
            send[g * batch + i] = chosen[i * stride : i * stride + capacity]

    def dispatch_high():
        table = jnp.concatenate([places(i, codes_high) for i in range(near)], axis=0).astype(bf16)
        chosen = jnp.dot(table, normed_high[...], preferred_element_type=f32).astype(bf16)
        rows[high, 0] = chosen[:capacity]
        for i in range(1, near):
            passed[i] = chosen[i * stride : i * stride + capacity]

    def column(row):
        square = (row.shape[1], row.shape[1])
        diagonal = lax.broadcasted_iota(jnp.int32, square, 0) == lax.broadcasted_iota(jnp.int32, square, 1)
        return jnp.sum(jnp.where(diagonal, row, 0.0), axis=1, keepdims=True)

    def combine(k):
        if stride == capacity:
            data = ret[k]
        else:
            packed[:capacity, :] = ret[k]
            data = packed[:stride]
        table = places(k)
        picked = lax.dot_general(table.astype(bf16), data, (((0,), (0,)), ((), ())), preferred_element_type=f32)
        expert_id = peer(k)
        weight_row = jnp.zeros((1, tok_count), f32)
        for c in range(routes.shape[0]):
            weight_row = weight_row + jnp.where(routes[c : c + 1] == expert_id, weights[c : c + 1], 0.0)
        combined[...] += picked * column(weight_row)

    for i in range(4):
        weight_copy(i).start()
    barrier = pltpu.get_barrier_semaphore()
    partners = [(peer(k), t) for k in range(1, experts)] + [(e, low), (e, high)]
    for device in partners:
        pl.semaphore_signal(barrier, inc=1, device_id=device, device_id_type=MESH)

    if stride != capacity:
        packed[...] = jnp.zeros_like(packed)
    hits = jnp.zeros((experts, tok_count), f32)
    for c in range(routes.shape[0]):
        named = lax.broadcasted_iota(jnp.int32, (experts, tok_count), 0) == routes[c : c + 1]
        hits = hits + named.astype(f32)
    square = (tok_count, tok_count)
    earlier = lax.broadcasted_iota(jnp.int32, square, 0) < lax.broadcasted_iota(jnp.int32, square, 1)
    rank = jnp.dot(hits.astype(bf16), earlier.astype(f32).astype(bf16), preferred_element_type=f32)
    codes[...] = jnp.where(hits > 0.0, rank, -1.0)
    token_float = tokens[...].astype(f32)
    mean = jnp.mean(token_float * token_float, axis=-1, keepdims=True)
    normed[...] = (token_float * lax.rsqrt(mean + EPS) * moe_gain[...]).astype(bf16)

    lax.fori_loop(0, experts // batch, lambda g, c: (dispatch(g), c)[1], 0)
    own_copy(0).start()
    pl.semaphore_wait(barrier, len(partners))

    if near:
        whole_block(1).start()
        whole_block(0).start()
        chunk(near).start()
        chunk(1).start()
    else:
        chunk(1).start()
    own_copy(0).wait()
    if near:
        beside(0).start()

    k_column = column(k_gain[...])
    for s in range(streams):
        kv_all[0, s, :HEAD_DIM] = turned(keys[s], k_column, cosine[...], sine[...])
        kv_all[0, s, HEAD_DIM:] = values[s]
    q_column = column(q_gain[...])
    for s in range(streams):
        for h in range(groups):
            head = turned(queries[s, h * HEAD_DIM : (h + 1) * HEAD_DIM], q_column, cosine[...], sine[...])
            q[s, :, h * positions : (h + 1) * positions] = head * bf16(HEAD_DIM**-0.5)
    best[...] = jnp.full_like(best, -1e30)
    total[...] = jnp.zeros_like(total)
    accum[...] = jnp.zeros_like(accum)
    combined[...] = jnp.zeros_like(combined)
    for i in range(4):
        weight_copy(i).wait()

    def forward(k):
        @pl.when(k > 0)
        def _():
            chunk(k).wait_recv()

        beside(k).start()

        @pl.when(k >= near)
        def _():
            across(k).start()

    def block_arrived():
        for i in range(2):
            whole_block(i).wait_recv()
        dispatch_high()

    def onward(k):
        @pl.when(k >= near)
        def _():
            across(k).wait_recv()

        if near:

            @pl.when(k < near)
            def _():
                passed_chunk(k).wait_recv()

        relay(k).start()

    def worked(k):
        beside(k).wait_recv()
        relay(k).wait_recv()
        expert(k)

    def pair_start(k):
        pair_far(k).start()
        pair_near(k).start()

    def half_sum(k):
        pair_far(k).wait_recv()
        gone[k] = (part[high, k].astype(f32) + pair[1, k].astype(f32)).astype(bf16)

    def whole_sum(k):
        pair_near(k).wait_recv()
        over(k).wait_recv()
        done[k] = (part[t, k].astype(f32) + pair[0, k].astype(f32) + seen[k].astype(f32)).astype(bf16)

    def back_start(k):
        @pl.when(k > 0)
        def _():
            back(k).start()

        @pl.when(k == 0)
        def _():
            own_copy(1).start()

    def back_arrived(k):
        @pl.when(k > 0)
        def _():
            back(k).wait_recv()

        @pl.when(k == 0)
        def _():
            own_copy(1).wait()

        combine(k)

    def kv_start(_):
        kv_side(0).start()
        lax.fori_loop(1, half // 2 + 1, lambda m, c: (kv_direct(m).start(), c)[1], 0)

    def kv_arrived(m):
        kv_direct(m).wait_recv()
        kv_side(m).start()

        @pl.when(m == half // 2)
        def _():
            lax.fori_loop(half // 2 + 1, half, lambda i, c: (kv_onward(i).start(), c)[1], 0)

    def attention(m):
        attend(2 * m)
        kv_side(m).wait_recv()
        attend(2 * m + 1)

    def projected(_):
        project()
        other(1).start()
        other(0).start()

    def other_half(_):
        other(1).wait_recv()
        gone_att[...] = (prod[high].astype(f32) + pair_att[1].astype(f32)).astype(bf16)

    acts = dict(
        R=forward, S=lambda k: chunk(k).start(), T=lambda _: block_arrived(), L=onward, X=worked, D=whole_sum,
        G=half_sum, P=pair_start, O=lambda k: over(k).start(), Q=lambda _: relay(0).start(), U=lambda k: passed_chunk(k).start(), B=back_start, K=kv_start,
        V=kv_arrived, A=attention, C=back_arrived, J=projected, H=other_half, I=lambda _: other(2).start(),
    )
    tables, slots = in_slots(schedule(experts, near))

    def step(i, carry):
        for name in RANKS:
            table = tables[name]
            if not table:
                continue
            number = jnp.int32(-1)
            for slot, value in table:
                number = jnp.where(i == slot, value, number)

            @pl.when(number >= 0)
            def _(name=name, number=number):
                acts[name](number)

        return carry

    lax.fori_loop(0, slots, step, 0)
    other(0).wait_recv()
    other(2).wait_recv()
    att[...] = (prod[t].astype(f32) + pair_att[0].astype(f32) + seen_att[...].astype(f32)).astype(bf16)
    routed[...] = combined[...].astype(bf16)

    def finish(k, carry):
        beside(k).wait_send()
        relay(k).wait_send()
        pair_far(k).wait_send()
        pair_near(k).wait_send()
        over(k).wait_send()

        @pl.when(k >= near)
        def _():
            across(k).wait_send()

        @pl.when(k >= 1)
        def _():
            back(k).wait_send()
            chunk(k).wait_send()


        @pl.when(k < half)
        def _():
            kv_side(k).wait_send()

        @pl.when((k >= 1) & (k < half))
        def _():
            kv_direct(k).wait_send()

        return carry

    lax.fori_loop(0, experts, finish, 0)
    if near:
        for k in range(1, near):
            passed_chunk(k).wait_send()
        for i in range(2):
            whole_block(i).wait_send()
    for i in range(3):
        other(i).wait_send()


def fused(experts, capacity, tokens, moe_gain, routes, weights, queries, keys, *rest):
    values, q_gain, k_gain, cosine, sine, out_weight, w_gate, w_up, w_down = rest
    like = tokens.dtype
    f32 = jnp.float32
    sem = pltpu.SemaphoreType.DMA((experts,))
    tok_count, features = tokens.shape
    streams, _, positions = keys.shape
    query_lanes = queries.shape[1] // HEAD_DIM * positions
    att = (positions // 4 * streams, features)
    stride = -(-capacity // 16) * 16
    block = (experts, capacity, features)
    shapes = [
        (block, like),
        ((4,) + block, like),
        ((4,) + block, like),
        ((2,) + block, like),
        (block, like),
        (block, like),
        (block, like),
        (block, like),
        ((4 * stride, features), like),
        (tokens.shape, like),
        ((experts, streams, 2 * HEAD_DIM, positions), like),
        ((streams, HEAD_DIM, query_lanes), like),
        ((4,) + att, like),
        ((2,) + att, like),
        (att, like),
        (att, like),
        ((streams, HEAD_DIM, query_lanes), f32),
        ((streams, 1, query_lanes), f32),
        ((streams, 1, query_lanes), f32),
        ((experts, tok_count), f32),
        (tokens.shape, f32),
        (out_weight.shape, like),
        (w_gate.shape, like),
        (w_up.shape, like),
        (w_down.shape, like),
        ((4, capacity, features), like),
        (tokens.shape, like),
        ((experts, tok_count), f32),
    ]
    vmem = pl.BlockSpec(memory_space=pltpu.VMEM)
    hbm = pl.BlockSpec(memory_space=pl.ANY)
    return pl.pallas_call(
        functools.partial(fused_kernel, experts, capacity),
        out_shape=(jax.ShapeDtypeStruct(tokens.shape, like), jax.ShapeDtypeStruct(att, like)),
        in_specs=[vmem] * 11 + [hbm] * 4,
        out_specs=(vmem, vmem),
        scratch_shapes=[pltpu.VMEM(shape, dtype) for shape, dtype in shapes]
        + [pltpu.SemaphoreType.DMA((4,)), pltpu.SemaphoreType.DMA((2,))]
        + [sem] * 20
        + [pltpu.SemaphoreType.DMA((3,))] * 2
        + [pltpu.SemaphoreType.DMA((4,))] * 2
        + [pltpu.SemaphoreType.DMA((2,))] * 2,
        name="fused",
        compiler_params=pltpu.CompilerParams(
            collective_id=1, has_side_effects=True, vmem_limit_bytes=62 * 2**20
        ),
    )(tokens, moe_gain, routes, weights, queries, keys, values, q_gain, k_gain, cosine, sine,
      out_weight, w_gate, w_up, w_down)


def per_device(
    queries,
    keys,
    values,
    query_gain,
    key_gain,
    out_weight,
    moe_tokens,
    moe_gain,
    routes,
    route_weight,
    w_gate,
    w_up,
    w_down,
):
    pos_count, seq_count = queries.shape[:2]
    positions = lax.axis_index("ep") * pos_count + jnp.arange(pos_count, dtype=jnp.int32)
    inverse = THETA ** (-jnp.arange(QUARTER, dtype=jnp.float32) / QUARTER)
    grid_row = (positions // GRID_W).astype(jnp.float32)
    grid_col = (positions % GRID_W).astype(jnp.float32)
    angles = jnp.concatenate([inverse[:, None] * grid_row, inverse[:, None] * grid_col], axis=0)
    kv_local = keys.shape[2] // HEAD_DIM
    streams = seq_count * kv_local
    experts = lax.axis_size("ep")
    capacity = max(2, (3 * moe_tokens.shape[0] * routes.shape[1] + 2 * experts - 1) // (2 * experts))

    def by_feature(data):
        return jnp.transpose(data, (1, 2, 0)).reshape(streams, -1, pos_count)

    routed, attended = fused(
        experts,
        capacity,
        moe_tokens,
        moe_gain[None, :],
        routes.T,
        route_weight.T,
        by_feature(queries),
        by_feature(keys),
        by_feature(values),
        query_gain[None, :],
        key_gain[None, :],
        jnp.cos(angles),
        jnp.sin(angles),
        out_weight,
        w_gate[0],
        w_up[0],
        w_down[0],
    )
    quarter = pos_count // lax.axis_size("tp")
    attended = jnp.transpose(attended.reshape(seq_count, quarter, -1), (1, 0, 2))
    return (attended, routed)


def solution(mesh):
    in_specs = (
        P("ep", None, "tp"),
        P("ep", None, "tp"),
        P("ep", None, "tp"),
        P(),
        P(),
        P("tp", None),
        P(("ep", "tp"), None),
        P(),
        P(("ep", "tp"), None),
        P(("ep", "tp"), None),
        P("ep", None, "tp"),
        P("ep", None, "tp"),
        P("ep", "tp", None),
    )
    out_specs = (P(("ep", "tp"), None, None), P(("ep", "tp"), None))
    return jax.shard_map(
        per_device, mesh=mesh, in_specs=in_specs, out_specs=out_specs, check_vma=False
    )
```

```python
import functools
import math
import math

import jax
import jax.numpy as jnp
from jax import lax
from jax.experimental import pallas as pl
from jax.experimental.pallas import tpu as pltpu
from jax.sharding import PartitionSpec as P

HEAD_DIM = 64
QUARTER = HEAD_DIM // 4
GRID_W = 64

EPS = 1e-06
THETA = 10000.0

MESH = pl.DeviceIdType.MESH


def exclusive_or(a, b, count):
    result = 0
    bit = 1
    while bit < count:
        result = result + (a // bit + b // bit) % 2 * bit
        bit *= 2
    return result


RANKS = "RSTLXDGPOQUBKVACFJHI"


def schedule(experts, near):
    half = experts // 2
    far = list(range(near, experts))
    if near == 4 and experts == 8:
        listed = (
            "R1 K0 S5 T0", "R4 S6 Q0 U1", "V1 X0 P0 G0", "O0 L4 L1 X1", "P1 V2 G1 O1", "R5 S7 S2 U2",
            "X4 P4 V3 G4", "O4 A0 L5 R6", "S3 U3 X5 P5", "A1 G5 O5 D4", "B4 R7 L6 A2", "X6 P6 D5 B5",
            "G6 O6 R2 L2", "X2 P2 A3 G2", "O2 L7 X7 P7", "J0 G7 O7 D6", "B6 R3 L3 X3", "P3 H0 G3 O3",
            "D7 B7 D1 B1", "I0 D2 B2 C4", "C5 D0 B0 D3", "B3 C6 C0 C1", "C2 C7 F0 C3",
        )
        return [(word[0], int(word[1:])) for word in " ".join(listed).split()]
    program = []
    for i in range(experts + 5):
        stages = (("R", 0), ("S", -2), ("L", 1), ("X", 2), ("D", 5), ("G", 3), ("P", 2), ("O", 3), ("B", 5))
        for name, delay in stages:
            if 0 <= i - delay < experts:
                program.append((name, i - delay))
    program.append(("K", 0))
    program += [("V", m) for m in range(1, half)] + [("A", m) for m in range(half)]
    return program + [("J", 0), ("H", 0), ("I", 0)] + [("C", k) for k in range(experts)] + [("F", 0)]


def in_slots(program):
    tables, slot, last = {name: [] for name in RANKS}, 0, -1
    for name, number in program:
        rank = RANKS.index(name)
        if rank <= last:
            slot += 1
        last = rank
        tables[name].append((slot, number))
    return tables, slot + 1


def turned(block, gain, cosine, sine):
    block = block.astype(jnp.float32)
    mean = jnp.mean(block * block, axis=0, keepdims=True)
    normed = block * lax.rsqrt(mean + EPS) * gain
    parts = []
    for axis in range(2):
        first = normed[2 * axis * QUARTER : (2 * axis + 1) * QUARTER]
        second = normed[(2 * axis + 1) * QUARTER : (2 * axis + 2) * QUARTER]
        c = cosine[axis * QUARTER : (axis + 1) * QUARTER]
        s = sine[axis * QUARTER : (axis + 1) * QUARTER]
        parts += [first * c - second * s, second * c + first * s]
    return jnp.concatenate(parts, axis=0).astype(jnp.bfloat16)


def fused_kernel(
    experts, capacity, tokens, moe_gain, routes, weights, queries_hbm, keys_hbm, values_hbm, q_gain, k_gain,
    out_weight_hbm, w_gate_hbm, w_up_hbm, w_down_hbm, routed, att, *scratch
):
    (send, rows, part, pair, gone, seen, done, ret, packed, normed) = scratch[:10]
    (kv_all, q, prod, pair_att, gone_att, seen_att, accum, best, total, codes, combined) = scratch[10:21]
    (out_weight, w_gate, w_up, w_down, passed, normed_high, codes_high) = scratch[21:28]
    (queries, keys, values, w_sem, own) = scratch[28:33]
    (a_send, a_recv, y_send, y_recv, l_send, l_recv, m_send, m_recv, k_send, k_recv, x_send, x_recv) = scratch[33:45]
    (f_send, f_recv, n_send, n_recv, c_send, c_recv, b_send, b_recv, o_send, o_recv) = scratch[45:55]
    (p_send, p_recv, t_send, t_recv) = scratch[55:]
    f32, bf16 = jnp.float32, jnp.bfloat16
    e, t = lax.axis_index("ep"), lax.axis_index("tp")
    low, high = t + 1 - 2 * (t % 2), (t + 2) % 4
    low_high = (low + 2) % 4
    half = experts // 2
    side = e + 1 - 2 * (e % 2)
    stride = packed.shape[0] // 4
    streams = kv_all.shape[1]
    positions = kv_all.shape[3]
    groups = q.shape[2] // positions
    tok_count = tokens.shape[0]

    def peer(k):
        return exclusive_or(e, k, experts)

    def remote(src, dst, s, r, device):
        return pltpu.make_async_remote_copy(
            src_ref=src, dst_ref=dst, send_sem=s, recv_sem=r, device_id=device, device_id_type=MESH
        )

    def kv_direct(m):
        return remote(kv_all.at[0], kv_all.at[2 * m], k_send.at[m], k_recv.at[m], (peer(2 * m), t))

    def kv_onward(m):
        return remote(kv_all.at[half], kv_all.at[2 * m], k_send.at[m], k_recv.at[m], (peer(2 * m - half), t))

    def kv_side(m):
        return remote(kv_all.at[2 * m], kv_all.at[2 * m + 1], x_send.at[m], x_recv.at[m], (side, t))

    def chunk(k):
        return remote(send.at[k], rows.at[t, k], a_send.at[k], a_recv.at[k], (peer(k), t))

    def passed_chunk(k):
        return remote(passed.at[k], rows.at[high, k], p_send.at[k], p_recv.at[k], (peer(k), t))

    def whole_block(i):
        src, dst = ((normed, normed_high), (codes, codes_high))[i]
        return remote(src, dst, t_send.at[i], t_recv.at[i], (e, high))

    def across(k):
        block = rows.at[t, k]
        return remote(block, block, y_send.at[k], y_recv.at[k], (e, high))

    def beside(k):
        block = rows.at[t, k]
        return remote(block, block, l_send.at[k], l_recv.at[k], (e, low))

    def relay(k):
        block = rows.at[high, k]
        return remote(block, block, m_send.at[k], m_recv.at[k], (e, low))

    def pair_far(k):
        return remote(part.at[low_high, k], pair.at[1, k], f_send.at[k], f_recv.at[k], (e, low))

    def pair_near(k):
        return remote(part.at[low, k], pair.at[0, k], n_send.at[k], n_recv.at[k], (e, low))

    def over(k):
        return remote(gone.at[k], seen.at[k], c_send.at[k], c_recv.at[k], (e, high))

    def back(k):
        return remote(done.at[k], ret.at[k], b_send.at[k], b_recv.at[k], (peer(k), t))

    def other(i):
        if i < 2:
            return remote(prod.at[(low, low_high)[i]], pair_att.at[i], o_send.at[i], o_recv.at[i], (e, low))
        return remote(gone_att, seen_att, o_send.at[i], o_recv.at[i], (e, high))

    def own_copy(i):
        if i == 0:
            return pltpu.make_async_copy(send.at[0], rows.at[t, 0], own.at[0])
        return pltpu.make_async_copy(done.at[0], ret.at[0], own.at[1])

    def weight_copy(i):
        pairs = ((keys_hbm, keys), (values_hbm, values), (queries_hbm, queries), (out_weight_hbm, out_weight))
        pairs += ((w_gate_hbm, w_gate), (w_up_hbm, w_up), (w_down_hbm, w_down))
        return pltpu.make_async_copy(pairs[i][0], pairs[i][1], w_sem.at[i])

    def attend(j):
        for s in range(streams):
            key_block = kv_all[j, s, :HEAD_DIM]
            value_block = kv_all[j, s, HEAD_DIM:]
            scores = lax.dot_general(key_block, q[s], (((0,), (0,)), ((), ())), preferred_element_type=f32)
            old = best[s]
            new = jnp.maximum(old, jnp.max(scores, axis=0, keepdims=True))
            factor = jnp.exp(old - new)
            expo = jnp.exp(scores - new)
            best[s] = new
            total[s] = total[s] * factor + jnp.sum(expo, axis=0, keepdims=True)
            added = jnp.dot(value_block, expo.astype(bf16), preferred_element_type=f32)
            accum[s] = accum[s] * factor + added

    def project():
        rows_out = positions * streams
        place = lax.broadcasted_iota(jnp.int32, (positions, rows_out), 1)
        position = lax.broadcasted_iota(jnp.int32, (positions, rows_out), 0)
        laid = jnp.zeros((groups * HEAD_DIM, rows_out), f32)
        for s in range(streams):
            mixed = (accum[s] / total[s]).astype(bf16)
            stacked = jnp.concatenate([mixed[:, g * positions : (g + 1) * positions] for g in range(groups)], axis=0)
            chosen = (place == position * streams + s).astype(f32).astype(bf16)
            laid = laid + jnp.dot(stacked, chosen, preferred_element_type=f32)
        for b in range(4):
            block = laid[:, b * rows_out // 4 : (b + 1) * rows_out // 4].astype(bf16)
            product = lax.dot_general(block, out_weight[...], (((0,), (0,)), ((), ())), preferred_element_type=f32)
            prod[b] = product.astype(bf16)

    def expert(k):
        for b in range(4):
            packed[b * stride : b * stride + capacity, :] = rows[b, k]
        data = packed[...]
        gate = jnp.dot(data, w_gate[...], preferred_element_type=f32)
        up = jnp.dot(data, w_up[...], preferred_element_type=f32)
        hidden = (gate * (1.0 / (1.0 + jnp.exp(-gate))) * up).astype(bf16)
        result = jnp.dot(hidden, w_down[...], preferred_element_type=f32).astype(bf16)
        for b in range(4):
            part[b, k] = result[b * stride : b * stride + capacity]

    def places(k, table=codes):
        row = table[pl.ds(peer(k), 1), :]
        slot = lax.broadcasted_iota(jnp.int32, (stride, tok_count), 0).astype(f32)
        return (slot == row).astype(f32)

    batch = min(experts, 4)
    near = 4 if experts == 8 and 4 * capacity > tok_count else 0
    far = experts - near

    def dispatch(g):
        table = jnp.concatenate([places(g * batch + i) for i in range(batch)], axis=0).astype(bf16)
        chosen = jnp.dot(table, normed[...], preferred_element_type=f32).astype(bf16)
        for i in range(batch):
            send[g * batch + i] = chosen[i * stride : i * stride + capacity]

    def dispatch_high():
        table = jnp.concatenate([places(i, codes_high) for i in range(near)], axis=0).astype(bf16)
        chosen = jnp.dot(table, normed_high[...], preferred_element_type=f32).astype(bf16)
        rows[high, 0] = chosen[:capacity]
        for i in range(1, near):
            passed[i] = chosen[i * stride : i * stride + capacity]

    def column(row):
        square = (row.shape[1], row.shape[1])
        diagonal = lax.broadcasted_iota(jnp.int32, square, 0) == lax.broadcasted_iota(jnp.int32, square, 1)
        return jnp.sum(jnp.where(diagonal, row, 0.0), axis=1, keepdims=True)

    def combine(k):
        if stride == capacity:
            data = ret[k]
        else:
            packed[:capacity, :] = ret[k]
            data = packed[:stride]
        table = places(k)
        picked = lax.dot_general(table.astype(bf16), data, (((0,), (0,)), ((), ())), preferred_element_type=f32)
        expert_id = peer(k)
        weight_row = jnp.zeros((1, tok_count), f32)
        for c in range(routes.shape[0]):
            weight_row = weight_row + jnp.where(routes[c : c + 1] == expert_id, weights[c : c + 1], 0.0)
        combined[...] += picked * column(weight_row)

    for i in range(7):
        weight_copy(i).start()
    barrier = pltpu.get_barrier_semaphore()
    partners = [(peer(k), t) for k in range(1, experts)] + [(e, low), (e, high)]
    for device in partners:
        pl.semaphore_signal(barrier, inc=1, device_id=device, device_id_type=MESH)

    if stride != capacity:
        packed[...] = jnp.zeros_like(packed)
    hits = jnp.zeros((experts, tok_count), f32)
    for c in range(routes.shape[0]):
        named = lax.broadcasted_iota(jnp.int32, (experts, tok_count), 0) == routes[c : c + 1]
        hits = hits + named.astype(f32)
    square = (tok_count, tok_count)
    earlier = lax.broadcasted_iota(jnp.int32, square, 0) < lax.broadcasted_iota(jnp.int32, square, 1)
    rank = jnp.dot(hits.astype(bf16), earlier.astype(f32).astype(bf16), preferred_element_type=f32)
    codes[...] = jnp.where(hits > 0.0, rank, -1.0)
    token_float = tokens[...].astype(f32)
    mean = jnp.mean(token_float * token_float, axis=-1, keepdims=True)
    normed[...] = (token_float * lax.rsqrt(mean + EPS) * moe_gain[...]).astype(bf16)

    lax.fori_loop(0, experts // batch, lambda g, c: (dispatch(g), c)[1], 0)
    own_copy(0).start()
    pl.semaphore_wait(barrier, len(partners))

    if near:
        whole_block(1).start()
        whole_block(0).start()
        chunk(near).start()
        chunk(1).start()
    else:
        chunk(1).start()
    own_copy(0).wait()
    if near:
        beside(0).start()

    for i in range(3):
        weight_copy(i).wait()
    shape = (2 * QUARTER, positions)
    turn_row = lax.broadcasted_iota(jnp.int32, shape, 0)
    power = (turn_row % QUARTER).astype(f32) * (-math.log(THETA) / QUARTER)
    place = e * positions + lax.broadcasted_iota(jnp.int32, shape, 1)
    grid = jnp.where(turn_row < QUARTER, place // GRID_W, place % GRID_W).astype(f32)
    angles = grid * jnp.exp(power)
    cosine, sine = jnp.cos(angles), jnp.sin(angles)
    k_column = column(k_gain[...])
    for s in range(streams):
        kv_all[0, s, :HEAD_DIM] = turned(keys[s], k_column, cosine, sine)
        kv_all[0, s, HEAD_DIM:] = values[s]
    q_column = column(q_gain[...])
    flat = queries[...].reshape(positions * streams, groups * HEAD_DIM)
    row = lax.broadcasted_iota(jnp.int32, (positions * streams, positions), 0)
    position = lax.broadcasted_iota(jnp.int32, (positions * streams, positions), 1)
    for s in range(streams):
        chosen = (row == position * streams + s).astype(f32).astype(bf16)
        by_feature = lax.dot_general(flat, chosen, (((0,), (0,)), ((), ())), preferred_element_type=f32)
        for h in range(groups):
            head = turned(by_feature[h * HEAD_DIM : (h + 1) * HEAD_DIM], q_column, cosine, sine)
            q[s, :, h * positions : (h + 1) * positions] = head * bf16(HEAD_DIM**-0.5)
    best[...] = jnp.full_like(best, -1e30)
    total[...] = jnp.zeros_like(total)
    accum[...] = jnp.zeros_like(accum)
    combined[...] = jnp.zeros_like(combined)
    for i in range(3, 7):
        weight_copy(i).wait()

    def forward(k):
        @pl.when(k > 0)
        def _():
            chunk(k).wait_recv()

        beside(k).start()

        @pl.when(k >= near)
        def _():
            across(k).start()

    def block_arrived():
        for i in range(2):
            whole_block(i).wait_recv()
        dispatch_high()

    def onward(k):
        @pl.when(k >= near)
        def _():
            across(k).wait_recv()

        if near:

            @pl.when(k < near)
            def _():
                passed_chunk(k).wait_recv()

        relay(k).start()

    def worked(k):
        beside(k).wait_recv()
        relay(k).wait_recv()
        expert(k)

    def pair_start(k):
        pair_far(k).start()
        pair_near(k).start()

    def half_sum(k):
        pair_far(k).wait_recv()
        gone[k] = (part[high, k].astype(f32) + pair[1, k].astype(f32)).astype(bf16)

    def whole_sum(k):
        pair_near(k).wait_recv()
        over(k).wait_recv()
        done[k] = (part[t, k].astype(f32) + pair[0, k].astype(f32) + seen[k].astype(f32)).astype(bf16)

    def back_start(k):
        @pl.when(k > 0)
        def _():
            back(k).start()

        @pl.when(k == 0)
        def _():
            own_copy(1).start()

    def back_arrived(k):
        @pl.when(k > 0)
        def _():
            back(k).wait_recv()

        @pl.when(k == 0)
        def _():
            own_copy(1).wait()

        combine(k)

    def kv_start(_):
        kv_side(0).start()
        lax.fori_loop(1, half // 2 + 1, lambda m, c: (kv_direct(m).start(), c)[1], 0)

    def kv_arrived(m):
        kv_direct(m).wait_recv()
        kv_side(m).start()

        @pl.when(m == half // 2)
        def _():
            lax.fori_loop(half // 2 + 1, half, lambda i, c: (kv_onward(i).start(), c)[1], 0)

    def attention(m):
        attend(2 * m)
        kv_side(m).wait_recv()
        attend(2 * m + 1)

    def projected(_):
        project()
        other(1).start()
        other(0).start()

    def other_half(_):
        other(1).wait_recv()
        gone_att[...] = (prod[high].astype(f32) + pair_att[1].astype(f32)).astype(bf16)

    def finish_attended(_):
        other(0).wait_recv()
        other(2).wait_recv()
        summed = prod[t].astype(f32) + pair_att[0].astype(f32) + seen_att[...].astype(f32)
        att[...] = summed.astype(bf16).reshape(att.shape)

    acts = dict(
        R=forward, S=lambda k: chunk(k).start(), T=lambda _: block_arrived(), L=onward, X=worked, D=whole_sum,
        G=half_sum, P=pair_start, O=lambda k: over(k).start(), Q=lambda _: relay(0).start(), U=lambda k: passed_chunk(k).start(), B=back_start, K=kv_start,
        V=kv_arrived, A=attention, C=back_arrived, J=projected, H=other_half, I=lambda _: other(2).start(), F=finish_attended,
    )
    tables, slots = in_slots(schedule(experts, near))

    def step(i, carry):
        for name in RANKS:
            table = tables[name]
            if not table:
                continue
            number = jnp.int32(-1)
            for slot, value in table:
                number = jnp.where(i == slot, value, number)

            @pl.when(number >= 0)
            def _(name=name, number=number):
                acts[name](number)

        return carry

    lax.fori_loop(0, slots, step, 0)
    routed[...] = combined[...].astype(bf16)

    def finish(k, carry):
        beside(k).wait_send()
        relay(k).wait_send()
        pair_far(k).wait_send()
        pair_near(k).wait_send()
        over(k).wait_send()

        @pl.when(k >= near)
        def _():
            across(k).wait_send()

        @pl.when(k >= 1)
        def _():
            back(k).wait_send()
            chunk(k).wait_send()


        @pl.when(k < half)
        def _():
            kv_side(k).wait_send()

        @pl.when((k >= 1) & (k < half))
        def _():
            kv_direct(k).wait_send()

        return carry

    lax.fori_loop(0, experts, finish, 0)
    if near:
        for k in range(1, near):
            passed_chunk(k).wait_send()
        for i in range(2):
            whole_block(i).wait_send()
    for i in range(3):
        other(i).wait_send()


def fused(experts, capacity, tokens, moe_gain, routes, weights, queries, keys, *rest):
    values, q_gain, k_gain, out_weight, w_gate, w_up, w_down = rest
    like = tokens.dtype
    f32 = jnp.float32
    sem = pltpu.SemaphoreType.DMA((experts,))
    tok_count, features = tokens.shape
    streams, _, positions = keys.shape
    query_lanes = queries.shape[2] // HEAD_DIM * positions
    att = (positions // 4 * streams, features)
    att_out = (positions // 4, streams, features)
    stride = -(-capacity // 16) * 16
    block = (experts, capacity, features)
    shapes = [
        (block, like),
        ((4,) + block, like),
        ((4,) + block, like),
        ((2,) + block, like),
        (block, like),
        (block, like),
        (block, like),
        (block, like),
        ((4 * stride, features), like),
        (tokens.shape, like),
        ((experts, streams, 2 * HEAD_DIM, positions), like),
        ((streams, HEAD_DIM, query_lanes), like),
        ((4,) + att, like),
        ((2,) + att, like),
        (att, like),
        (att, like),
        ((streams, HEAD_DIM, query_lanes), f32),
        ((streams, 1, query_lanes), f32),
        ((streams, 1, query_lanes), f32),
        ((experts, tok_count), f32),
        (tokens.shape, f32),
        (out_weight.shape, like),
        (w_gate.shape, like),
        (w_up.shape, like),
        (w_down.shape, like),
        ((4, capacity, features), like),
        (tokens.shape, like),
        ((experts, tok_count), f32),
        (queries.shape, like),
        (keys.shape, like),
        (values.shape, like),
    ]
    vmem = pl.BlockSpec(memory_space=pltpu.VMEM)
    hbm = pl.BlockSpec(memory_space=pl.ANY)
    return pl.pallas_call(
        functools.partial(fused_kernel, experts, capacity),
        out_shape=(pltpu.VMEM(tokens.shape, like), pltpu.VMEM(att_out, like)),
        in_specs=[vmem] * 4 + [hbm] * 3 + [vmem] * 2 + [hbm] * 4,
        out_specs=(vmem, vmem),
        scratch_shapes=[pltpu.VMEM(shape, dtype) for shape, dtype in shapes]
        + [pltpu.SemaphoreType.DMA((7,)), pltpu.SemaphoreType.DMA((2,))]
        + [sem] * 20
        + [pltpu.SemaphoreType.DMA((3,))] * 2
        + [pltpu.SemaphoreType.DMA((4,))] * 2
        + [pltpu.SemaphoreType.DMA((2,))] * 2,
        name="fused",
        compiler_params=pltpu.CompilerParams(
            collective_id=1, has_side_effects=True, vmem_limit_bytes=62 * 2**20
        ),
    )(tokens, moe_gain, routes, weights, queries, keys, values, q_gain, k_gain,
      out_weight, w_gate, w_up, w_down)


def carry_kernel(*refs):
    leave = [pltpu.make_async_copy(refs[i], refs[2 + i], refs[4].at[i]) for i in range(2)]
    for copy in leave:
        copy.start()
    for copy in leave:
        copy.wait()


def carry(*arrays):
    shapes = [jax.ShapeDtypeStruct(array.shape, array.dtype) for array in arrays]
    return pl.pallas_call(
        carry_kernel,
        out_shape=tuple(shapes),
        in_specs=[pl.BlockSpec(memory_space=pltpu.VMEM)] * 2,
        out_specs=(pl.BlockSpec(memory_space=pl.ANY),) * 2,
        scratch_shapes=[pltpu.SemaphoreType.DMA((2,))],
        name="carry",
    )(*[pltpu.with_memory_space_constraint(array, pltpu.VMEM) for array in arrays])


def per_device(
    queries,
    keys,
    values,
    query_gain,
    key_gain,
    out_weight,
    moe_tokens,
    moe_gain,
    routes,
    route_weight,
    w_gate,
    w_up,
    w_down,
):
    pos_count, seq_count = queries.shape[:2]
    kv_local = keys.shape[2] // HEAD_DIM
    streams = seq_count * kv_local
    experts = lax.axis_size("ep")
    capacity = max(2, (3 * moe_tokens.shape[0] * routes.shape[1] + 2 * experts - 1) // (2 * experts))

    def by_feature(data):
        return jnp.transpose(data, (1, 2, 0)).reshape(streams, -1, pos_count)

    routed, attended = fused(
        experts,
        capacity,
        moe_tokens,
        moe_gain[None, :],
        routes.T,
        route_weight.T,
        queries,
        by_feature(keys),
        by_feature(values),
        query_gain[None, :],
        key_gain[None, :],
        out_weight,
        w_gate[0],
        w_up[0],
        w_down[0],
    )
    return carry(attended, routed)


def solution(mesh):
    in_specs = (
        P("ep", None, "tp"),
        P("ep", None, "tp"),
        P("ep", None, "tp"),
        P(),
        P(),
        P("tp", None),
        P(("ep", "tp"), None),
        P(),
        P(("ep", "tp"), None),
        P(("ep", "tp"), None),
        P("ep", None, "tp"),
        P("ep", None, "tp"),
        P("ep", "tp", None),
    )
    out_specs = (P(("ep", "tp"), None, None), P(("ep", "tp"), None))
    return jax.shard_map(
        per_device, mesh=mesh, in_specs=in_specs, out_specs=out_specs, check_vma=False
    )
```

```python
import functools
import math
import math

import jax
import jax.numpy as jnp
from jax import lax
from jax.experimental import pallas as pl
from jax.experimental.pallas import tpu as pltpu
from jax.sharding import PartitionSpec as P

HEAD_DIM = 64
QUARTER = HEAD_DIM // 4
GRID_W = 64

EPS = 1e-06
THETA = 10000.0

MESH = pl.DeviceIdType.MESH


def exclusive_or(a, b, count):
    result = 0
    bit = 1
    while bit < count:
        result = result + (a // bit + b // bit) % 2 * bit
        bit *= 2
    return result


RANKS = "RSTLXDGPOQUBKVACFJHI"


def schedule(experts, near):
    half = experts // 2
    far = list(range(near, experts))
    if near == 4 and experts == 8:
        listed = (
            "R1 K0 T0 R4", "S5 Q0 U1 V1", "X0 P0 G0 O0", "L4 S6 L1 X1", "P1 V2 G1 O1", "S2 U2 X4 R5",
            "S7 P4 G4 V3", "O4 A0 L5 R6", "S3 U3 X5 P5", "A1 G5 O5 D4", "B4 D1 B1 D0", "B0 R7 L6 A2",
            "X6 P6 D5 B5", "G6 O6 R2 L2", "X2 P2 A3 G2", "O2 L7 X7 P7", "J0 G7 O7 D6", "B6 R3 L3 X3",
            "P3 H0 G3 O3", "D7 B7 I0 D2", "B2 C4 C5 D3", "B3 C6 C0 C1", "C2 C7 F0 C3",
        )
        return [(word[0], int(word[1:])) for word in " ".join(listed).split()]
    program = []
    for i in range(experts + 5):
        stages = (("R", 0), ("S", -2), ("L", 1), ("X", 2), ("D", 5), ("G", 3), ("P", 2), ("O", 3), ("B", 5))
        for name, delay in stages:
            if 0 <= i - delay < experts:
                program.append((name, i - delay))
    program.append(("K", 0))
    program += [("V", m) for m in range(1, half)] + [("A", m) for m in range(half)]
    return program + [("J", 0), ("H", 0), ("I", 0)] + [("C", k) for k in range(experts)] + [("F", 0)]


def in_slots(program):
    tables, slot, last = {name: [] for name in RANKS}, 0, -1
    for name, number in program:
        rank = RANKS.index(name)
        if rank <= last:
            slot += 1
        last = rank
        tables[name].append((slot, number))
    return tables, slot + 1


def turned(block, gain, cosine, sine):
    block = block.astype(jnp.float32)
    mean = jnp.mean(block * block, axis=0, keepdims=True)
    normed = block * lax.rsqrt(mean + EPS) * gain
    parts = []
    for axis in range(2):
        first = normed[2 * axis * QUARTER : (2 * axis + 1) * QUARTER]
        second = normed[(2 * axis + 1) * QUARTER : (2 * axis + 2) * QUARTER]
        c = cosine[axis * QUARTER : (axis + 1) * QUARTER]
        s = sine[axis * QUARTER : (axis + 1) * QUARTER]
        parts += [first * c - second * s, second * c + first * s]
    return jnp.concatenate(parts, axis=0).astype(jnp.bfloat16)


def fused_kernel(
    experts, capacity, tokens, moe_gain, routes, weights, queries_hbm, keys_hbm, values_hbm, q_gain, k_gain,
    out_weight_hbm, w_gate_hbm, w_up_hbm, w_down_hbm, routed, att, *scratch
):
    (send, rows, part, pair, gone, seen, done, ret, packed, normed) = scratch[:10]
    (kv_all, q, prod, pair_att, gone_att, seen_att, accum, best, total, codes, combined) = scratch[10:21]
    (out_weight, w_gate, w_up, w_down, passed, normed_high, codes_high) = scratch[21:28]
    (queries, keys, values, w_sem, own) = scratch[28:33]
    (a_send, a_recv, y_send, y_recv, l_send, l_recv, m_send, m_recv, k_send, k_recv, x_send, x_recv) = scratch[33:45]
    (f_send, f_recv, n_send, n_recv, c_send, c_recv, b_send, b_recv, o_send, o_recv) = scratch[45:55]
    (p_send, p_recv, t_send, t_recv) = scratch[55:]
    f32, bf16 = jnp.float32, jnp.bfloat16
    e, t = lax.axis_index("ep"), lax.axis_index("tp")
    low, high = t + 1 - 2 * (t % 2), (t + 2) % 4
    low_high = (low + 2) % 4
    half = experts // 2
    side = e + 1 - 2 * (e % 2)
    stride = packed.shape[0] // 4
    streams = kv_all.shape[1]
    positions = kv_all.shape[3]
    groups = q.shape[2] // positions
    tok_count = tokens.shape[0]

    def peer(k):
        return exclusive_or(e, k, experts)

    def remote(src, dst, s, r, device):
        return pltpu.make_async_remote_copy(
            src_ref=src, dst_ref=dst, send_sem=s, recv_sem=r, device_id=device, device_id_type=MESH
        )

    def kv_direct(m):
        return remote(kv_all.at[0], kv_all.at[2 * m], k_send.at[m], k_recv.at[m], (peer(2 * m), t))

    def kv_onward(m):
        return remote(kv_all.at[half], kv_all.at[2 * m], k_send.at[m], k_recv.at[m], (peer(2 * m - half), t))

    def kv_side(m):
        return remote(kv_all.at[2 * m], kv_all.at[2 * m + 1], x_send.at[m], x_recv.at[m], (side, t))

    def chunk(k):
        return remote(send.at[k], rows.at[t, k], a_send.at[k], a_recv.at[k], (peer(k), t))

    def passed_chunk(k):
        return remote(passed.at[k], rows.at[high, k], p_send.at[k], p_recv.at[k], (peer(k), t))

    def whole_block(i):
        src, dst = ((normed, normed_high), (codes, codes_high))[i]
        return remote(src, dst, t_send.at[i], t_recv.at[i], (e, high))

    def across(k):
        block = rows.at[t, k]
        return remote(block, block, y_send.at[k], y_recv.at[k], (e, high))

    def beside(k):
        block = rows.at[t, k]
        return remote(block, block, l_send.at[k], l_recv.at[k], (e, low))

    def relay(k):
        block = rows.at[high, k]
        return remote(block, block, m_send.at[k], m_recv.at[k], (e, low))

    def pair_far(k):
        return remote(part.at[low_high, k], pair.at[1, k], f_send.at[k], f_recv.at[k], (e, low))

    def pair_near(k):
        return remote(part.at[low, k], pair.at[0, k], n_send.at[k], n_recv.at[k], (e, low))

    def over(k):
        return remote(gone.at[k], seen.at[k], c_send.at[k], c_recv.at[k], (e, high))

    def back(k):
        return remote(done.at[k], ret.at[k], b_send.at[k], b_recv.at[k], (peer(k), t))

    def other(i):
        if i < 2:
            return remote(prod.at[(low, low_high)[i]], pair_att.at[i], o_send.at[i], o_recv.at[i], (e, low))
        return remote(gone_att, seen_att, o_send.at[i], o_recv.at[i], (e, high))

    def own_copy(i):
        if i == 0:
            return pltpu.make_async_copy(send.at[0], rows.at[t, 0], own.at[0])
        return pltpu.make_async_copy(done.at[0], ret.at[0], own.at[1])

    def weight_copy(i):
        pairs = ((keys_hbm, keys), (values_hbm, values), (queries_hbm, queries), (out_weight_hbm, out_weight))
        pairs += ((w_gate_hbm, w_gate), (w_up_hbm, w_up), (w_down_hbm, w_down))
        return pltpu.make_async_copy(pairs[i][0], pairs[i][1], w_sem.at[i])

    def attend(j):
        for s in range(streams):
            key_block = kv_all[j, s, :HEAD_DIM]
            value_block = kv_all[j, s, HEAD_DIM:]
            scores = lax.dot_general(key_block, q[s], (((0,), (0,)), ((), ())), preferred_element_type=f32)
            old = best[s]
            new = jnp.maximum(old, jnp.max(scores, axis=0, keepdims=True))
            factor = jnp.exp(old - new)
            expo = jnp.exp(scores - new)
            best[s] = new
            total[s] = total[s] * factor + jnp.sum(expo, axis=0, keepdims=True)
            added = jnp.dot(value_block, expo.astype(bf16), preferred_element_type=f32)
            accum[s] = accum[s] * factor + added

    def project():
        rows_out = positions * streams
        place = lax.broadcasted_iota(jnp.int32, (positions, rows_out), 1)
        position = lax.broadcasted_iota(jnp.int32, (positions, rows_out), 0)
        laid = jnp.zeros((groups * HEAD_DIM, rows_out), f32)
        for s in range(streams):
            mixed = (accum[s] / total[s]).astype(bf16)
            stacked = jnp.concatenate([mixed[:, g * positions : (g + 1) * positions] for g in range(groups)], axis=0)
            chosen = (place == position * streams + s).astype(f32).astype(bf16)
            laid = laid + jnp.dot(stacked, chosen, preferred_element_type=f32)
        for b in range(4):
            block = laid[:, b * rows_out // 4 : (b + 1) * rows_out // 4].astype(bf16)
            product = lax.dot_general(block, out_weight[...], (((0,), (0,)), ((), ())), preferred_element_type=f32)
            prod[b] = product.astype(bf16)

    def expert(k):
        for b in range(4):
            packed[b * stride : b * stride + capacity, :] = rows[b, k]
        data = packed[...]
        gate = jnp.dot(data, w_gate[...], preferred_element_type=f32)
        up = jnp.dot(data, w_up[...], preferred_element_type=f32)
        hidden = (gate * (1.0 / (1.0 + jnp.exp(-gate))) * up).astype(bf16)
        result = jnp.dot(hidden, w_down[...], preferred_element_type=f32).astype(bf16)
        for b in range(4):
            part[b, k] = result[b * stride : b * stride + capacity]

    def places(k, table=codes):
        row = table[pl.ds(peer(k), 1), :]
        slot = lax.broadcasted_iota(jnp.int32, (stride, tok_count), 0).astype(f32)
        return (slot == row).astype(f32)

    batch = min(experts, 4)
    near = 4 if experts == 8 and 4 * capacity > tok_count else 0
    far = experts - near

    def dispatch(g):
        table = jnp.concatenate([places(g * batch + i) for i in range(batch)], axis=0).astype(bf16)
        chosen = jnp.dot(table, normed[...], preferred_element_type=f32).astype(bf16)
        for i in range(batch):
            send[g * batch + i] = chosen[i * stride : i * stride + capacity]

    def dispatch_high():
        table = jnp.concatenate([places(i, codes_high) for i in range(near)], axis=0).astype(bf16)
        chosen = jnp.dot(table, normed_high[...], preferred_element_type=f32).astype(bf16)
        rows[high, 0] = chosen[:capacity]
        for i in range(1, near):
            passed[i] = chosen[i * stride : i * stride + capacity]

    def column(row):
        square = (row.shape[1], row.shape[1])
        diagonal = lax.broadcasted_iota(jnp.int32, square, 0) == lax.broadcasted_iota(jnp.int32, square, 1)
        return jnp.sum(jnp.where(diagonal, row, 0.0), axis=1, keepdims=True)

    def combine(k):
        if stride == capacity:
            data = ret[k]
        else:
            packed[:capacity, :] = ret[k]
            data = packed[:stride]
        table = places(k)
        picked = lax.dot_general(table.astype(bf16), data, (((0,), (0,)), ((), ())), preferred_element_type=f32)
        expert_id = peer(k)
        weight_row = jnp.zeros((1, tok_count), f32)
        for c in range(routes.shape[0]):
            weight_row = weight_row + jnp.where(routes[c : c + 1] == expert_id, weights[c : c + 1], 0.0)
        combined[...] += picked * column(weight_row)

    for i in range(7):
        weight_copy(i).start()
    barrier = pltpu.get_barrier_semaphore()
    partners = [(peer(k), t) for k in range(1, experts)] + [(e, low), (e, high)]
    for device in partners:
        pl.semaphore_signal(barrier, inc=1, device_id=device, device_id_type=MESH)

    if stride != capacity:
        packed[...] = jnp.zeros_like(packed)
    hits = jnp.zeros((experts, tok_count), f32)
    for c in range(routes.shape[0]):
        named = lax.broadcasted_iota(jnp.int32, (experts, tok_count), 0) == routes[c : c + 1]
        hits = hits + named.astype(f32)
    square = (tok_count, tok_count)
    earlier = lax.broadcasted_iota(jnp.int32, square, 0) < lax.broadcasted_iota(jnp.int32, square, 1)
    rank = jnp.dot(hits.astype(bf16), earlier.astype(f32).astype(bf16), preferred_element_type=f32)
    codes[...] = jnp.where(hits > 0.0, rank, -1.0)
    token_float = tokens[...].astype(f32)
    mean = jnp.mean(token_float * token_float, axis=-1, keepdims=True)
    normed[...] = (token_float * lax.rsqrt(mean + EPS) * moe_gain[...]).astype(bf16)

    lax.fori_loop(0, experts // batch, lambda g, c: (dispatch(g), c)[1], 0)
    own_copy(0).start()
    pl.semaphore_wait(barrier, len(partners))

    if near:
        whole_block(1).start()
        whole_block(0).start()
        chunk(near).start()
        chunk(1).start()
    else:
        chunk(1).start()
    own_copy(0).wait()
    if near:
        beside(0).start()

    for i in range(3):
        weight_copy(i).wait()
    shape = (2 * QUARTER, positions)
    turn_row = lax.broadcasted_iota(jnp.int32, shape, 0)
    power = (turn_row % QUARTER).astype(f32) * (-math.log(THETA) / QUARTER)
    place = e * positions + lax.broadcasted_iota(jnp.int32, shape, 1)
    grid = jnp.where(turn_row < QUARTER, place // GRID_W, place % GRID_W).astype(f32)
    angles = grid * jnp.exp(power)
    cosine, sine = jnp.cos(angles), jnp.sin(angles)
    k_column = column(k_gain[...])
    for s in range(streams):
        kv_all[0, s, :HEAD_DIM] = turned(keys[s], k_column, cosine, sine)
        kv_all[0, s, HEAD_DIM:] = values[s]
    q_column = column(q_gain[...])
    flat = queries[...].reshape(positions * streams, groups * HEAD_DIM)
    row = lax.broadcasted_iota(jnp.int32, (positions * streams, positions), 0)
    position = lax.broadcasted_iota(jnp.int32, (positions * streams, positions), 1)
    for s in range(streams):
        chosen = (row == position * streams + s).astype(f32).astype(bf16)
        by_feature = lax.dot_general(flat, chosen, (((0,), (0,)), ((), ())), preferred_element_type=f32)
        for h in range(groups):
            head = turned(by_feature[h * HEAD_DIM : (h + 1) * HEAD_DIM], q_column, cosine, sine)
            q[s, :, h * positions : (h + 1) * positions] = head * bf16(HEAD_DIM**-0.5)
    best[...] = jnp.full_like(best, -1e30)
    total[...] = jnp.zeros_like(total)
    accum[...] = jnp.zeros_like(accum)
    combined[...] = jnp.zeros_like(combined)
    for i in range(3, 7):
        weight_copy(i).wait()

    def forward(k):
        @pl.when(k > 0)
        def _():
            chunk(k).wait_recv()

        beside(k).start()

        @pl.when(k >= near)
        def _():
            across(k).start()

    def block_arrived():
        for i in range(2):
            whole_block(i).wait_recv()
        dispatch_high()

    def onward(k):
        @pl.when(k >= near)
        def _():
            across(k).wait_recv()

        if near:

            @pl.when(k < near)
            def _():
                passed_chunk(k).wait_recv()

        relay(k).start()

    def worked(k):
        beside(k).wait_recv()
        relay(k).wait_recv()
        expert(k)

    def pair_start(k):
        pair_far(k).start()
        pair_near(k).start()

    def half_sum(k):
        pair_far(k).wait_recv()
        gone[k] = (part[high, k].astype(f32) + pair[1, k].astype(f32)).astype(bf16)

    def whole_sum(k):
        pair_near(k).wait_recv()
        over(k).wait_recv()
        done[k] = (part[t, k].astype(f32) + pair[0, k].astype(f32) + seen[k].astype(f32)).astype(bf16)

    def back_start(k):
        @pl.when(k > 0)
        def _():
            back(k).start()

        @pl.when(k == 0)
        def _():
            own_copy(1).start()

    def back_arrived(k):
        @pl.when(k > 0)
        def _():
            back(k).wait_recv()

        @pl.when(k == 0)
        def _():
            own_copy(1).wait()

        combine(k)

    def kv_start(_):
        kv_side(0).start()
        lax.fori_loop(1, half // 2 + 1, lambda m, c: (kv_direct(m).start(), c)[1], 0)

    def kv_arrived(m):
        kv_direct(m).wait_recv()
        kv_side(m).start()

        @pl.when(m == half // 2)
        def _():
            lax.fori_loop(half // 2 + 1, half, lambda i, c: (kv_onward(i).start(), c)[1], 0)

    def attention(m):
        attend(2 * m)
        kv_side(m).wait_recv()
        attend(2 * m + 1)

    def projected(_):
        project()
        other(1).start()
        other(0).start()

    def other_half(_):
        other(1).wait_recv()
        gone_att[...] = (prod[high].astype(f32) + pair_att[1].astype(f32)).astype(bf16)

    def finish_attended(_):
        other(0).wait_recv()
        other(2).wait_recv()
        summed = prod[t].astype(f32) + pair_att[0].astype(f32) + seen_att[...].astype(f32)
        att[...] = summed.astype(bf16).reshape(att.shape)

    acts = dict(
        R=forward, S=lambda k: chunk(k).start(), T=lambda _: block_arrived(), L=onward, X=worked, D=whole_sum,
        G=half_sum, P=pair_start, O=lambda k: over(k).start(), Q=lambda _: relay(0).start(), U=lambda k: passed_chunk(k).start(), B=back_start, K=kv_start,
        V=kv_arrived, A=attention, C=back_arrived, J=projected, H=other_half, I=lambda _: other(2).start(), F=finish_attended,
    )
    tables, slots = in_slots(schedule(experts, near))

    def step(i, carry):
        for name in RANKS:
            table = tables[name]
            if not table:
                continue
            number = jnp.int32(-1)
            for slot, value in table:
                number = jnp.where(i == slot, value, number)

            @pl.when(number >= 0)
            def _(name=name, number=number):
                acts[name](number)

        return carry

    lax.fori_loop(0, slots, step, 0)
    routed[...] = combined[...].astype(bf16)

    def finish(k, carry):
        beside(k).wait_send()
        relay(k).wait_send()
        pair_far(k).wait_send()
        pair_near(k).wait_send()
        over(k).wait_send()

        @pl.when(k >= near)
        def _():
            across(k).wait_send()

        @pl.when(k >= 1)
        def _():
            back(k).wait_send()
            chunk(k).wait_send()


        @pl.when(k < half)
        def _():
            kv_side(k).wait_send()

        @pl.when((k >= 1) & (k < half))
        def _():
            kv_direct(k).wait_send()

        return carry

    lax.fori_loop(0, experts, finish, 0)
    if near:
        for k in range(1, near):
            passed_chunk(k).wait_send()
        for i in range(2):
            whole_block(i).wait_send()
    for i in range(3):
        other(i).wait_send()


def fused(experts, capacity, tokens, moe_gain, routes, weights, queries, keys, *rest):
    values, q_gain, k_gain, out_weight, w_gate, w_up, w_down = rest
    like = tokens.dtype
    f32 = jnp.float32
    sem = pltpu.SemaphoreType.DMA((experts,))
    tok_count, features = tokens.shape
    streams, _, positions = keys.shape
    query_lanes = queries.shape[2] // HEAD_DIM * positions
    att = (positions // 4 * streams, features)
    att_out = (positions // 4, streams, features)
    stride = -(-capacity // 16) * 16
    block = (experts, capacity, features)
    shapes = [
        (block, like),
        ((4,) + block, like),
        ((4,) + block, like),
        ((2,) + block, like),
        (block, like),
        (block, like),
        (block, like),
        (block, like),
        ((4 * stride, features), like),
        (tokens.shape, like),
        ((experts, streams, 2 * HEAD_DIM, positions), like),
        ((streams, HEAD_DIM, query_lanes), like),
        ((4,) + att, like),
        ((2,) + att, like),
        (att, like),
        (att, like),
        ((streams, HEAD_DIM, query_lanes), f32),
        ((streams, 1, query_lanes), f32),
        ((streams, 1, query_lanes), f32),
        ((experts, tok_count), f32),
        (tokens.shape, f32),
        (out_weight.shape, like),
        (w_gate.shape, like),
        (w_up.shape, like),
        (w_down.shape, like),
        ((4, capacity, features), like),
        (tokens.shape, like),
        ((experts, tok_count), f32),
        (queries.shape, like),
        (keys.shape, like),
        (values.shape, like),
    ]
    vmem = pl.BlockSpec(memory_space=pltpu.VMEM)
    hbm = pl.BlockSpec(memory_space=pl.ANY)
    return pl.pallas_call(
        functools.partial(fused_kernel, experts, capacity),
        out_shape=(pltpu.VMEM(tokens.shape, like), pltpu.VMEM(att_out, like)),
        in_specs=[vmem] * 4 + [hbm] * 3 + [vmem] * 2 + [hbm] * 4,
        out_specs=(vmem, vmem),
        scratch_shapes=[pltpu.VMEM(shape, dtype) for shape, dtype in shapes]
        + [pltpu.SemaphoreType.DMA((7,)), pltpu.SemaphoreType.DMA((2,))]
        + [sem] * 20
        + [pltpu.SemaphoreType.DMA((3,))] * 2
        + [pltpu.SemaphoreType.DMA((4,))] * 2
        + [pltpu.SemaphoreType.DMA((2,))] * 2,
        name="fused",
        compiler_params=pltpu.CompilerParams(
            collective_id=1, has_side_effects=True, vmem_limit_bytes=62 * 2**20
        ),
    )(tokens, moe_gain, routes, weights, queries, keys, values, q_gain, k_gain,
      out_weight, w_gate, w_up, w_down)


def carry_kernel(*refs):
    leave = [pltpu.make_async_copy(refs[i], refs[2 + i], refs[4].at[i]) for i in range(2)]
    for copy in leave:
        copy.start()
    for copy in leave:
        copy.wait()


def carry(*arrays):
    shapes = [jax.ShapeDtypeStruct(array.shape, array.dtype) for array in arrays]
    return pl.pallas_call(
        carry_kernel,
        out_shape=tuple(shapes),
        in_specs=[pl.BlockSpec(memory_space=pltpu.VMEM)] * 2,
        out_specs=(pl.BlockSpec(memory_space=pl.ANY),) * 2,
        scratch_shapes=[pltpu.SemaphoreType.DMA((2,))],
        name="carry",
    )(*[pltpu.with_memory_space_constraint(array, pltpu.VMEM) for array in arrays])


def per_device(
    queries,
    keys,
    values,
    query_gain,
    key_gain,
    out_weight,
    moe_tokens,
    moe_gain,
    routes,
    route_weight,
    w_gate,
    w_up,
    w_down,
):
    pos_count, seq_count = queries.shape[:2]
    kv_local = keys.shape[2] // HEAD_DIM
    streams = seq_count * kv_local
    experts = lax.axis_size("ep")
    capacity = max(2, (3 * moe_tokens.shape[0] * routes.shape[1] + 2 * experts - 1) // (2 * experts))

    def by_feature(data):
        return jnp.transpose(data, (1, 2, 0)).reshape(streams, -1, pos_count)

    routed, attended = fused(
        experts,
        capacity,
        moe_tokens,
        moe_gain[None, :],
        routes.T,
        route_weight.T,
        queries,
        by_feature(keys),
        by_feature(values),
        query_gain[None, :],
        key_gain[None, :],
        out_weight,
        w_gate[0],
        w_up[0],
        w_down[0],
    )
    return carry(attended, routed)


def solution(mesh):
    in_specs = (
        P("ep", None, "tp"),
        P("ep", None, "tp"),
        P("ep", None, "tp"),
        P(),
        P(),
        P("tp", None),
        P(("ep", "tp"), None),
        P(),
        P(("ep", "tp"), None),
        P(("ep", "tp"), None),
        P("ep", None, "tp"),
        P("ep", None, "tp"),
        P("ep", "tp", None),
    )
    out_specs = (P(("ep", "tp"), None, None), P(("ep", "tp"), None))
    return jax.shard_map(
        per_device, mesh=mesh, in_specs=in_specs, out_specs=out_specs, check_vma=False
    )
```
